32 devices in a mesh: sp: 4 (over y, x), tp: 8 (over z, core).
Axes of the slice: x: 2, y: 2, z: 4, core: 2. Of those that a mesh axis runs over, the one named last changes fastest.
Arguments:
- resid: bfloat16 [2048, 2048], P(('sp', 'tp')), may hold values from -6 to 6
- query_a: bfloat16 [2048, 16, 128], P('sp', 'tp'), may hold values from -16 to 16
- key_a: bfloat16 [2048, 16, 128], P('sp', 'tp'), may hold values from -16 to 16
- value_a: bfloat16 [2048, 16, 128], P('sp', 'tp'), may hold values from -6 to 6
- query_b: bfloat16 [2048, 16, 64], P('sp', 'tp'), may hold values from -16 to 16
- key_b: bfloat16 [2048, 16, 64], P('sp', 'tp'), may hold values from -16 to 16
- value_b: bfloat16 [2048, 16, 64], P('sp', 'tp'), may hold values from -6 to 6
- mix_a: float32 [16], P('tp'), may hold values from 0.3 to 0.8
- mix_b: float32 [16], P('tp'), may hold values from 0.3 to 0.8
- head_gain_a: float32 [128], replicated, may hold values from 0.1 to 1.9
- head_gain_b: float32 [64], replicated, may hold values from 0.1 to 1.9
- proj_a: bfloat16 [2048, 2048], P('tp'), may hold values from -0.109375 to 0.109375
- proj_b: bfloat16 [1024, 2048], P('tp'), may hold values from -0.109375 to 0.109375
- norm_gain: float32 [2048], replicated, may hold values from 0.1 to 1.9
- route_ids: int32 [2048, 2], P(('sp', 'tp')), may hold values from 0 to 3, all different within a row; in each aligned block of 64 rows (0 to 63, 64 to 127, ...) at most 48 rows name the same one
- route_weights: float32 [2048, 2], P(('sp', 'tp')), may hold values from 0.2 to 1
- expert_gate: bfloat16 [4, 2048, 6144], P('sp', None, 'tp'), may hold values from -0.125 to 0.125
- expert_up: bfloat16 [4, 2048, 6144], P('sp', None, 'tp'), may hold values from -0.125 to 0.125
- expert_down: bfloat16 [4, 6144, 2048], P('sp', 'tp'), may hold values from -0.078125 to 0.078125
Outputs:
- out: bfloat16 [2048, 2048], P(('sp', 'tp'))
The draws below stay inside these ranges and needn't reach their ends.
Inputs may be any that keep to these rules, and one draw needn't show every extreme that they name: `route_ids`: each row names 2 different experts. Within the rows of one device (aligned blocks of 64 rows) no expert is named by more than 48 rows, and in every draw some device's block names some expert exactly 48 times.
All inputs are finite; a program needn't handle non-finite values.
Results may differ from the reference program's by a relative error of at most 0.02.
Values may be sent and summed in bfloat16 or wider, within the bound.
A program may use at most 128 MiB of HBM per device.

```python
import math
import jax
import jax.numpy as jnp
import numpy as np
from jax import lax

D = 2048
HEADS_A = 16
QK_A = 64
V_A = 128
HEADS_B = 16
QK_B = 32
V_B = 64
FF = 6144
TOP = 2
SEQ_DEV = 512
EXPERTS = 4
TOK_DEV = 64
CAP = 48
TOKENS = 2048
N_TP = 8


def drawn_pair(key, heads, width):
    shape = (TOKENS, heads, 2 * width)
    query = jnp.clip(jax.random.normal(jax.random.fold_in(key, 21), shape, jnp.float32) * 1.3, -8.0, 8.0)
    keys = jnp.clip(jax.random.normal(jax.random.fold_in(key, 22), shape, jnp.float32) * 1.3, -8.0, 8.0)
    return (query, keys)


def draw_query_a(key, part):
    return drawn_pair(jax.random.fold_in(key, 1), HEADS_A, QK_A)[0].astype(jnp.bfloat16)


def draw_key_a(key, part):
    return drawn_pair(jax.random.fold_in(key, 1), HEADS_A, QK_A)[1].astype(jnp.bfloat16)


def draw_query_b(key, part):
    return drawn_pair(jax.random.fold_in(key, 2), HEADS_B, QK_B)[0].astype(jnp.bfloat16)


def draw_key_b(key, part):
    return drawn_pair(jax.random.fold_in(key, 2), HEADS_B, QK_B)[1].astype(jnp.bfloat16)


def level_of(stream_key, shape, split, smallest, largest):
    def one(axis_at, parts):
        steps = jax.random.uniform(jax.random.fold_in(jax.random.fold_in(stream_key, 6), axis_at), (parts,), jnp.float32, smallest / len(split), largest / len(split))
        return jnp.repeat(jnp.exp(steps), shape[axis_at] // parts).reshape((-1,) + (1,) * (len(shape) - axis_at - 1))

    loudness = one(*split[0])
    for cut in split[1:]:
        loudness = loudness * one(*cut)
    return loudness


def routed_block(key, own, number, rows, number_of, top, most, skew):
    order = jax.random.permutation(key, number_of)
    packed, common = shares(number_of, rows * top, most, skew, True), shares(number_of, rows * top, most, skew, False)
    places = jnp.arange(number_of)

    def named(tallies, turn):
        used = int((tallies > 0).sum())
        fixed = max(1, used // 4)
        moved = fixed + (places - fixed + turn * (used - fixed)) % max(1, number_of - fixed)
        return jnp.zeros((number_of,), jnp.int32).at[order[jnp.where(places < fixed, places, moved)]].set(jnp.asarray(tallies, jnp.int32))

    tallies = jnp.where(number % 4 == 0, named(packed, number // 4), named(common, number - number // 4 - 1))
    mixed = jax.random.permutation(jax.random.fold_in(own, 3), number_of)
    source_of, sink = mixed[0:number_of // 2 * 2:2], mixed[1:number_of // 2 * 2:2]
    margin = jnp.minimum(tallies[source_of] - 1, most - tallies[sink]) // 2
    margin = jnp.where((source_of == order[0]) | (sink == order[0]) | (tallies[sink] == 0), 0, jnp.maximum(margin, 0))
    moved = jax.random.randint(jax.random.fold_in(own, 4), (number_of // 2,), 0, 1 << 20) % (margin + 1)
    tallies = tallies.at[source_of].add(-moved).at[sink].add(moved)
    items = jnp.searchsorted(jnp.cumsum(tallies), jnp.arange(rows * top), side="right").astype(jnp.int32)
    table = items.reshape(top, rows).T
    table = table[jax.random.permutation(jax.random.fold_in(own, 1), rows)]
    turn = jax.random.randint(jax.random.fold_in(own, 2), (rows, 1), 0, top)
    return jnp.take_along_axis(table, (jnp.arange(top)[None, :] + turn) % top, axis=1)


def shares(number_of, total, reach, skew, full):
    loads = [(1 << 20) // math.isqrt(grade ** skew) + 1 for grade in range(1, number_of + 1)]
    largest = reach if full else min(reach, max(-(-total // number_of), total * loads[0] // sum(loads)))
    least = 1 if total - largest >= number_of - 1 else 0
    given, spare = [largest] + [least] * (number_of - 1), total - largest - least * (number_of - 1)
    while spare > 0:
        movable = [i for i in range(1, number_of) if given[i] < largest] or [i for i in range(1, number_of) if given[i] < reach]
        mass, remaining = sum([loads[i] for i in movable]), spare
        for i in movable:
            more = min(reach - given[i], max(1, remaining * loads[i] // mass), spare)
            given[i] = given[i] + more
            spare = spare - more
    return np.array(given)


def gaussian(stream_key, dims, scale, most, shards=(), held_as=jnp.bfloat16):
    drawn = jax.random.normal(stream_key, dims, jnp.float32) * scale
    if len(shards) > 0:
        drawn = level_of(stream_key, dims, shards, -0.22, 0.18) * drawn
    return jnp.clip(drawn, min=-most, max=most).astype(held_as)


def setup_inputs(seed: int = 0) -> dict:
    streams_of = jax.random.split(jax.random.key(seed), 20)
    resid = gaussian(streams_of[0], (TOKENS, D), 1.0, 6.0, ((0, 32),))
    query_a = draw_query_a(jax.random.fold_in(streams_of[19], 71), 0)
    key_a = draw_key_a(jax.random.fold_in(streams_of[19], 71), 0)
    value_a = gaussian(streams_of[3], (TOKENS, HEADS_A, V_A), 1.0, 6.0, ((0, 4), (1, 8)))
    query_b = draw_query_b(jax.random.fold_in(streams_of[19], 71), 0)
    key_b = draw_key_b(jax.random.fold_in(streams_of[19], 71), 0)
    value_b = gaussian(streams_of[6], (TOKENS, HEADS_B, V_B), 1.0, 6.0, ((0, 4), (1, 8)))
    mix_a = jnp.clip(0.3 + 0.5 * jax.random.uniform(streams_of[7], (HEADS_A,), jnp.float32) ** level_of(streams_of[7], (HEADS_A,), ((0, 8),), -0.2, 0.2), 0.3, 0.8)
    mix_b = jnp.clip(0.3 + 0.5 * jax.random.uniform(streams_of[8], (HEADS_B,), jnp.float32) ** level_of(streams_of[8], (HEADS_B,), ((0, 8),), -0.2, 0.2), 0.3, 0.8)
    head_gain_a = jnp.clip(1.0 + 0.18 * jax.random.normal(streams_of[9], (V_A,), jnp.float32), 0.1, 1.9)
    head_gain_b = jnp.clip(1.0 + 0.18 * jax.random.normal(streams_of[10], (V_B,), jnp.float32), 0.1, 1.9)
    proj_a = gaussian(streams_of[11], (HEADS_A * V_A, D), (HEADS_A * V_A + HEADS_B * V_B) ** -0.5, 0.109375, ((0, 8),))
    proj_b = gaussian(streams_of[12], (HEADS_B * V_B, D), (HEADS_A * V_A + HEADS_B * V_B) ** -0.5, 0.109375, ((0, 8),))
    norm_gain = jnp.clip(1.0 + 0.18 * jax.random.normal(streams_of[13], (D,), jnp.float32), 0.1, 1.9)
    route_ids_keys = jax.random.split(jax.random.fold_in(streams_of[14], 1), TOKENS // TOK_DEV)
    route_ids_turns = jax.random.permutation(jax.random.fold_in(streams_of[14], 3), TOKENS // TOK_DEV)
    route_ids = jax.vmap(lambda own, number: routed_block(jax.random.fold_in(streams_of[14], 2), own, number, TOK_DEV, EXPERTS, TOP, CAP, 1))(route_ids_keys, route_ids_turns).reshape((TOKENS, TOP))
    route_weights = jnp.clip(0.2 + 0.8 * jax.random.uniform(streams_of[15], (TOKENS, TOP), jnp.float32) ** level_of(streams_of[15], (TOKENS, TOP), ((0, 32),), -0.2, 0.2), 0.2, 1.0)
    expert_gate = gaussian(streams_of[16], (EXPERTS, D, FF), D ** -0.5, 0.125, ((0, 4), (2, 8)))
    expert_up = gaussian(streams_of[17], (EXPERTS, D, FF), D ** -0.5, 0.125, ((0, 4), (2, 8)))
    expert_down = gaussian(streams_of[18], (EXPERTS, FF, D), FF ** -0.5, 0.078125, ((0, 4), (1, 8)))
    return {"resid": resid, "query_a": query_a, "key_a": key_a, "value_a": value_a, "query_b": query_b, "key_b": key_b, "value_b": value_b, "mix_a": mix_a, "mix_b": mix_b, "head_gain_a": head_gain_a, "head_gain_b": head_gain_b, "proj_a": proj_a, "proj_b": proj_b, "norm_gain": norm_gain, "route_ids": route_ids, "route_weights": route_weights, "expert_gate": expert_gate, "expert_up": expert_up, "expert_down": expert_down}


EPS = 1e-06
HEAD_SCALE = 1.0 - (0.8 - 0.6 * math.exp(-0.3))

def attend(query, key, value, mix, gain):
    length, heads, double = query.shape
    width = double // 2
    scale = 1.0 / math.sqrt(width)
    block_rows = SEQ_DEV // 2
    keys_float = key.astype(jnp.float32)
    values_float = value.astype(jnp.float32)
    key_pos = jnp.arange(length, dtype=jnp.int32)

    def one_block(index):
        first = index * block_rows
        block = lax.dynamic_slice_in_dim(query, first, block_rows, 0).astype(jnp.float32)
        query_pos = first + jnp.arange(block_rows, dtype=jnp.int32)
        allowed = key_pos[None, :] <= query_pos[:, None]
        results = []
        for which in range(2):
            scores = jnp.einsum('qhd,khd->hqk', block[:, :, which * width:(which + 1) * width], keys_float[:, :, which * width:(which + 1) * width]) * scale
            scores = jnp.where(allowed[None], scores, -jnp.inf)
            shifted = jnp.exp(scores - lax.optimization_barrier(jnp.max(scores, axis=2, keepdims=True)))
            sums = lax.optimization_barrier(jnp.sum(shifted, axis=2))
            rounded = lax.optimization_barrier(shifted.astype(jnp.bfloat16)).astype(jnp.float32)
            weighted = jnp.einsum('hqk,khv->qhv', rounded, values_float)
            results.append(weighted / jnp.transpose(sums)[:, :, None])
        return results[0] - mix[None, :, None] * results[1]
    mixed = lax.map(one_block, jnp.arange(length // block_rows, dtype=jnp.int32))
    mixed = mixed.reshape(length, heads, -1)
    normed = mixed * lax.rsqrt(lax.optimization_barrier(jnp.mean(mixed * mixed, axis=2, keepdims=True)) + EPS) * gain * HEAD_SCALE
    return normed.astype(jnp.bfloat16).reshape(length, -1)

def slot_numbers(route_rows, experts, capacity):
    count, top_count = route_rows.shape
    flat = route_rows.reshape(count * top_count)
    onehot = (flat[:, None] == jnp.arange(experts, dtype=jnp.int32)[None, :]).astype(jnp.int32)
    ranks = lax.optimization_barrier(jnp.sum((jnp.cumsum(onehot, axis=0) - onehot) * onehot, axis=1))
    return (flat * capacity + ranks).reshape(count, top_count)

def reference(resid, query_a, key_a, value_a, query_b, key_b, value_b, mix_a, mix_b, head_gain_a, head_gain_b, proj_a, proj_b, norm_gain, route_ids, route_weights, expert_gate, expert_up, expert_down):
    heads_a = attend(query_a, key_a, value_a, mix_a, head_gain_a)
    heads_b = attend(query_b, key_b, value_b, mix_b, head_gain_b)
    cols_a = heads_a.shape[1] // N_TP
    cols_b = heads_b.shape[1] // N_TP
    mixed = resid.astype(jnp.float32)
    for shard in range(N_TP):
        partial_sum = jnp.dot(heads_a[:, shard * cols_a:(shard + 1) * cols_a], proj_a[shard * cols_a:(shard + 1) * cols_a], preferred_element_type=jnp.float32)
        partial_sum = partial_sum + jnp.dot(heads_b[:, shard * cols_b:(shard + 1) * cols_b], proj_b[shard * cols_b:(shard + 1) * cols_b], preferred_element_type=jnp.float32)
        mixed = mixed + lax.optimization_barrier(partial_sum.astype(jnp.bfloat16)).astype(jnp.float32)
    normed = (mixed * lax.rsqrt(lax.optimization_barrier(jnp.mean(mixed * mixed, axis=1, keepdims=True)) + EPS) * norm_gain).astype(jnp.bfloat16)
    blocks = TOKENS // TOK_DEV
    local = jax.vmap(lambda rows_in: slot_numbers(rows_in, EXPERTS, CAP))(route_ids.reshape(blocks, TOK_DEV, TOP))
    row_index = (jnp.arange(blocks, dtype=jnp.int32)[:, None, None] * CAP + local % CAP).reshape(-1)
    expert_index = route_ids.reshape(-1)
    buffer = jnp.zeros((EXPERTS, blocks * CAP, D), jnp.bfloat16)
    buffer = buffer.at[expert_index, row_index].set(jnp.repeat(normed, TOP, axis=0))
    block_width = FF // N_TP

    def run_expert(operands):
        rows_in, gate_w, up_w, down_w = operands
        gate = jnp.dot(rows_in, gate_w, preferred_element_type=jnp.float32)
        upward = jnp.dot(rows_in, up_w, preferred_element_type=jnp.float32)
        hidden = (jax.nn.silu(gate) * upward).astype(jnp.bfloat16)
        summed = jnp.zeros((rows_in.shape[0], D), jnp.float32)
        for shard in range(N_TP):
            part = jnp.dot(hidden[:, shard * block_width:(shard + 1) * block_width], down_w[shard * block_width:(shard + 1) * block_width], preferred_element_type=jnp.float32)
            summed = summed + lax.optimization_barrier(part.astype(jnp.bfloat16)).astype(jnp.float32)
        return summed.astype(jnp.bfloat16)
    outputs = lax.map(run_expert, (buffer, expert_gate, expert_up, expert_down))
    picked = outputs[expert_index, row_index].reshape(TOKENS, TOP, D).astype(jnp.float32)
    result = mixed + lax.optimization_barrier(jnp.sum(route_weights[:, :, None] * picked, axis=1))
    return result.astype(jnp.bfloat16)
```

```python
import functools
import math

import jax
import jax.numpy as jnp
import numpy as np
from jax import lax
from jax.experimental import pallas as pl
from jax.experimental.pallas import tpu as pltpu
from jax.sharding import PartitionSpec as P

EPS = 1e-06
NEG = -1e30
HEAD_SCALE = 1.0 - (0.8 - 0.6 * math.exp(-0.3))
KEY_STEP = 512


def partner(value, axis, apart):
    return lax.ppermute(value, axis, [(i, i ^ 1 << apart) for i in range(lax.axis_size(axis))])


def rms_scaled(values, gain):
    return values * lax.rsqrt(jnp.mean(values * values, axis=-1, keepdims=True) + EPS) * gain


def slot_numbers(route_rows, experts, capacity):
    count, top_count = route_rows.shape
    flat = route_rows.reshape(count * top_count)
    onehot = (flat[:, None] == jnp.arange(experts, dtype=jnp.int32)[None, :]).astype(jnp.int32)
    ranks = jnp.sum((jnp.cumsum(onehot, axis=0) - onehot) * onehot, axis=1)
    return (flat * capacity + ranks).reshape(count, top_count)


def empty_map(count, heads, width):
    return (
        jnp.zeros((count, heads, width), jnp.float32),
        jnp.full((heads, count), NEG, jnp.float32),
        jnp.zeros((heads, count), jnp.float32),
    )


def empty_group(query, value):
    return (
        empty_map(query.shape[0], query.shape[1], value.shape[2]),
        empty_map(query.shape[0], query.shape[1], value.shape[2]),
    )


def map_update(state, query, keys, values, allowed, scale):
    weighted, maximum, sums = state
    scores = jnp.einsum("qhd,khd->hqk", query, keys, preferred_element_type=jnp.float32) * scale
    scores = jnp.where(allowed[None], scores, NEG)
    fresh = jnp.maximum(maximum, jnp.max(scores, axis=2))
    weights = jnp.where(allowed[None], jnp.exp(scores - fresh[:, :, None]), 0.0)
    factor = jnp.exp(maximum - fresh)
    sums = sums * factor + jnp.sum(weights, axis=2)
    added = jnp.einsum(
        "hqk,khv->qhv", weights.astype(jnp.bfloat16), values, preferred_element_type=jnp.float32
    )
    weighted = weighted * jnp.transpose(factor)[:, :, None] + added
    return (weighted, fresh, sums)


def group_update(states, query, keys, values, allowed):
    width = query.shape[2] // 2
    scale = 1.0 / math.sqrt(width)
    return tuple(
        (
            map_update(
                states[which],
                query[:, :, which * width : (which + 1) * width],
                keys[:, :, which * width : (which + 1) * width],
                values,
                allowed,
                scale,
            )
            for which in range(2)
        )
    )


def set_update(carry, queries, pieces):
    rows_a, rows_b, query_pos = queries
    piece_key_a, piece_value_a, piece_key_b, piece_value_b = pieces
    length = piece_key_a.shape[0]
    step = math.gcd(length, KEY_STEP)
    latest = query_pos[-1]

    def inner(index, states):
        first = index * step

        def compute(current):
            keys_a = lax.dynamic_slice_in_dim(piece_key_a, first, step, 0)
            values_a = lax.dynamic_slice_in_dim(piece_value_a, first, step, 0)
            keys_b = lax.dynamic_slice_in_dim(piece_key_b, first, step, 0)
            values_b = lax.dynamic_slice_in_dim(piece_value_b, first, step, 0)
            key_pos = first + jnp.arange(step, dtype=jnp.int32)
            allowed = key_pos[None, :] <= query_pos[:, None]
            return (
                group_update(current[0], rows_a, keys_a, values_a, allowed),
                group_update(current[1], rows_b, keys_b, values_b, allowed),
            )

        return lax.cond(first <= latest, compute, lambda current: current, states)

    return lax.fori_loop(0, length // step, inner, carry)


def finish_group(states, mix, gain):
    outputs = [state[0] / jnp.transpose(state[2])[:, :, None] for state in states]
    mixed = outputs[0] - mix[None, :, None] * outputs[1]
    normed = rms_scaled(mixed, gain) * HEAD_SCALE
    return normed.astype(jnp.bfloat16).reshape(mixed.shape[0], -1)


def greet(axis, ways):
    me = lax.axis_index(axis)
    barrier = pltpu.get_barrier_semaphore()
    for apart in range(1, ways):
        pl.semaphore_signal(
            barrier,
            inc=1,
            device_id={axis: lax.rem(me + apart, ways)},
            device_id_type=pl.DeviceIdType.MESH,
        )
    pl.semaphore_wait(barrier, ways - 1)


def heads_kernel(
    units,
    chunk,
    qa_ref,
    ka_ref,
    va_ref,
    qb_ref,
    kb_ref,
    vb_ref,
    par_ref,
    out_ref,
    got_q,
    got_k,
    got_v,
    heads,
    send_in,
    recv_in,
    send_out,
    recv_out,
):
    me = lax.axis_index("sp")
    ways, rows, wide = got_q.shape
    greet("sp", ways)
    refs = {"a": (qa_ref, ka_ref, va_ref), "b": (qb_ref, kb_ref, vb_ref)}

    def unit_source(unit, kind):
        group, head = units[unit]
        ref = refs[group][kind]
        return ref.at[:, head * wide : (head + 1) * wide] if group == "a" else ref

    def unit_copy(unit, kind, landing, slot):
        return pltpu.make_async_remote_copy(
            src_ref=unit_source(unit, kind),
            dst_ref=(got_q, got_k, got_v)[kind].at[landing],
            send_sem=send_in.at[kind, unit],
            recv_sem=recv_in.at[kind, slot],
            device_id={"sp": unit},
            device_id_type=pl.DeviceIdType.MESH,
        )

    for unit in range(ways):

        @pl.when(me != unit)
        def _():
            for kind in range(3):
                unit_copy(unit, kind, me, me).start()

        @pl.when(me == unit)
        def _():
            for kind in range(3):
                (got_q, got_k, got_v)[kind][unit] = unit_source(unit, kind)[...]

    for unit in range(ways):

        @pl.when(me != unit)
        def _():
            for kind in range(3):
                unit_copy(unit, kind, unit, unit).wait()

    par = par_ref[me]
    gain, mix = par[0:1, :], par[1:2, :]
    scale, share = par[2:3, 0:1], par[3:4, 0:1]
    valid = par[6:7, :]

    def result_copy(block):
        return pltpu.make_async_remote_copy(
            src_ref=heads.at[block],
            dst_ref=out_ref.at[me],
            send_sem=send_out.at[block],
            recv_sem=recv_out.at[me],
            device_id={"sp": block},
            device_id_type=pl.DeviceIdType.MESH,
        )

    for block in reversed(range(ways)):
        length = (block + 1) * rows

        @pl.loop(0, rows // chunk)
        def _(step):
            first = pl.multiple_of(step * chunk, chunk)
            query = got_q[block, pl.ds(first, chunk), :]
            keys = got_k[0 : block + 1].reshape(length, wide)
            values = got_v[0 : block + 1].reshape(length, wide)
            row = first + block * rows + lax.broadcasted_iota(jnp.int32, (chunk, rows), 0)
            col = block * rows + lax.broadcasted_iota(jnp.int32, (chunk, rows), 1)
            parts = []
            for which in range(2):
                picked = query * par[4 + which : 5 + which, :].astype(jnp.bfloat16)
                scores = lax.dot_general(
                    picked, keys, (((1,), (1,)), ((), ())), preferred_element_type=jnp.float32
                )
                last = jnp.where(col <= row, scores[:, block * rows :], NEG)
                if block:
                    scores = jnp.concatenate([scores[:, : block * rows], last], axis=1)
                else:
                    scores = last
                top = jnp.max(scores, axis=1, keepdims=True)
                weights = jnp.exp2((scores - top) * scale)
                sums = jnp.sum(weights, axis=1, keepdims=True)
                mixed = jnp.dot(
                    weights.astype(jnp.bfloat16), values, preferred_element_type=jnp.float32
                )
                parts.append(mixed / sums)
            mixed = parts[0] - mix * parts[1]
            square = jnp.sum(mixed * mixed * valid, axis=1, keepdims=True) * share
            heads[block, pl.ds(first, chunk), :] = (
                mixed * lax.rsqrt(square + EPS) * gain * HEAD_SCALE
            ).astype(jnp.bfloat16)

        @pl.when(me != block)
        def _():
            result_copy(block).start()

        @pl.when(me == block)
        def _():
            out_ref[block] = heads[block]

    for block in range(ways):

        @pl.when(me != block)
        def _():
            result_copy(block).wait_send()
            pltpu.make_async_remote_copy(
                src_ref=heads.at[block],
                dst_ref=out_ref.at[block],
                send_sem=send_out.at[block],
                recv_sem=recv_out.at[block],
                device_id={"sp": block},
                device_id_type=pl.DeviceIdType.MESH,
            ).wait_recv()


def whole_heads(query_a, key_a, value_a, query_b, key_b, value_b, mix_a, mix_b, gain_a, gain_b):
    ways = lax.axis_size("sp")
    heads_a, heads_b = query_a.shape[1], query_b.shape[1]
    rows, wide = query_a.shape[0], value_a.shape[2]
    order = [("a", h) for h in range(heads_a)]
    spot = heads_a // 2
    order = order[:spot] + [("b", h) for h in range(heads_b)] + order[spot:]
    fixed = np.zeros((ways, 8, wide), np.float32)
    for unit, (group, head) in enumerate(order):
        value_wide = value_a.shape[2] if group == "a" else value_b.shape[2]
        narrow = (query_a.shape[2] if group == "a" else query_b.shape[2]) // 2
        first = 0 if group == "a" else head * 2 * narrow
        fixed[unit, 2] = math.log2(math.e) / math.sqrt(narrow)
        fixed[unit, 3] = 1.0 / value_wide
        fixed[unit, 4, first : first + narrow] = 1.0
        fixed[unit, 5, first + narrow : first + 2 * narrow] = 1.0
        first = 0 if group == "a" else head * value_wide
        fixed[unit, 6, first : first + value_wide] = 1.0
    gains = jnp.stack(
        [gain_a if group == "a" else jnp.tile(gain_b, heads_b) for group, _ in order]
    )
    mixes = jnp.stack([(mix_a if group == "a" else mix_b)[head] for group, head in order])
    par = jnp.concatenate(
        [
            (gains * fixed[:, 6])[:, None, :],
            jnp.broadcast_to(mixes[:, None, None], (ways, 1, wide)),
            fixed[:, 2:],
        ],
        axis=1,
    )
    chunk = math.gcd(rows, 128)
    held = pltpu.VMEM((ways, rows, wide), jnp.bfloat16)
    got = pl.pallas_call(
        functools.partial(heads_kernel, order, chunk),
        out_shape=jax.ShapeDtypeStruct((ways, rows, wide), jnp.bfloat16),
        in_specs=[pl.BlockSpec(memory_space=pltpu.VMEM)] * 7,
        out_specs=pl.BlockSpec(memory_space=pltpu.VMEM),
        scratch_shapes=[
            held,
            held,
            held,
            held,
            pltpu.SemaphoreType.DMA((3, ways)),
            pltpu.SemaphoreType.DMA((3, ways)),
            pltpu.SemaphoreType.DMA((ways,)),
            pltpu.SemaphoreType.DMA((ways,)),
        ],
        compiler_params=pltpu.CompilerParams(
            collective_id=1, has_side_effects=True, vmem_limit_bytes=48 << 20
        ),
    )(
        query_a.reshape(rows, -1),
        key_a.reshape(rows, -1),
        value_a.reshape(rows, -1),
        query_b.reshape(rows, -1),
        key_b.reshape(rows, -1),
        value_b.reshape(rows, -1),
        par,
    )
    out_a = [got[at] for at, unit in enumerate(order) if unit[0] == "a"]
    out_b = [got[at] for at, unit in enumerate(order) if unit[0] == "b"]
    return jnp.concatenate(out_a, axis=1), functools.reduce(jnp.add, out_b)


def zigzag_heads(query_a, key_a, value_a, query_b, key_b, value_b, mix_a, mix_b, gain_a, gain_b):
    head_gain_a, head_gain_b = gain_a, gain_b
    seq_rows = query_a.shape[0]
    sp_ways = lax.axis_size("sp")
    place = lax.axis_index("sp")
    positions = place * seq_rows + jnp.arange(seq_rows, dtype=jnp.int32)
    levels = sp_ways.bit_length() - 1
    half = seq_rows // 2
    moved = jnp.concatenate(
        [query_a[half:].reshape(half, -1), query_b[half:].reshape(half, -1)], axis=1
    )
    for bit in range(levels):
        moved = partner(moved, "sp", bit)
    split_at = query_a.shape[1] * query_a.shape[2]
    far_a = moved[:, :split_at].reshape(half, query_a.shape[1], query_a.shape[2])
    far_b = moved[:, split_at:].reshape(half, query_b.shape[1], query_b.shape[2])
    far_pos = (sp_ways - 1 - place) * seq_rows + half + jnp.arange(half, dtype=jnp.int32)
    query_sets = ((query_a[:half], query_b[:half], positions[:half]), (far_a, far_b, far_pos))

    def fold_keys(carry, pieces):
        return tuple(
            (set_update(states, queries, pieces) for states, queries in zip(carry, query_sets))
        )

    initial = tuple(
        (
            (empty_group(queries[0], value_a), empty_group(queries[1], value_b))
            for queries in query_sets
        )
    )
    results = fold_keys(
        initial,
        (
            lax.all_gather(key_a, "sp", axis=0, tiled=True),
            lax.all_gather(value_a, "sp", axis=0, tiled=True),
            lax.all_gather(key_b, "sp", axis=0, tiled=True),
            lax.all_gather(value_b, "sp", axis=0, tiled=True),
        ),
    )
    finished = [
        (finish_group(states[0], mix_a, head_gain_a), finish_group(states[1], mix_b, head_gain_b))
        for states in results
    ]
    returned = jnp.concatenate([finished[1][0], finished[1][1]], axis=1)
    for bit in range(levels):
        returned = partner(returned, "sp", bit)
    width_a = finished[0][0].shape[1]
    heads_out_a = jnp.concatenate([finished[0][0], returned[:, :width_a]], axis=0)
    heads_out_b = jnp.concatenate([finished[0][1], returned[:, width_a:]], axis=0)
    return heads_out_a, heads_out_b


def remote(src, dst, send_sem, recv_sem, **where):
    return pltpu.make_async_remote_copy(
        src_ref=src,
        dst_ref=dst,
        send_sem=send_sem,
        recv_sem=recv_sem,
        device_id=where,
        device_id_type=pl.DeviceIdType.MESH,
    )


def greet_routes(places, chips):
    place, turn = lax.axis_index("sp"), lax.axis_index("tp")
    chip, core = lax.div(turn, 2), lax.rem(turn, 2)
    barrier = pltpu.get_barrier_semaphore()
    peers = [{"tp": 2 * chip + 1 - core}]
    peers += [{"tp": 2 * lax.rem(chip + apart, chips) + core} for apart in range(1, chips)]
    peers += [{"sp": lax.rem(place + apart, places)} for apart in range(1, places)]
    for peer in peers:
        pl.semaphore_signal(
            barrier, inc=1, device_id=peer, device_id_type=pl.DeviceIdType.MESH
        )
    pl.semaphore_wait(barrier, len(peers))


def flipped(value, apart):
    bit = 1
    while bit <= apart:
        if apart & bit:
            value = value + bit - 2 * bit * lax.rem(lax.div(value, bit), 2)
        bit *= 2
    return value


def route_table(ids, weights, cap):
    rows = ids.shape[0]
    lane = lax.broadcasted_iota(jnp.int32, (rows, 128), 1)
    hits = [ids[:, which : which + 1] == lane for which in range(2)]
    named = jnp.where(hits[0], 1.0, 0.0) + jnp.where(hits[1], 1.0, 0.0)
    above = lax.broadcasted_iota(jnp.int32, (rows, rows), 0)
    above = above > lax.broadcasted_iota(jnp.int32, (rows, rows), 1)
    ranks = jnp.dot(
        jnp.where(above, 1.0, 0.0).astype(jnp.bfloat16),
        named.astype(jnp.bfloat16),
        preferred_element_type=jnp.float32,
    )
    spots = ranks + (lane * cap).astype(jnp.float32)
    table = jnp.zeros((rows, 128), jnp.float32)
    for which in range(2):
        spot = jnp.sum(jnp.where(hits[which], spots, 0.0), axis=1, keepdims=True)
        table = jnp.where(lane == which, spot, table)
        table = jnp.where(lane == which + 2, weights[:, which : which + 1], table)
    table = jnp.concatenate([table, jnp.zeros((128 - rows, 128), jnp.float32)], axis=0)
    return table.T[0:8, :]


def experts_kernel(
    places,
    chips,
    cap,
    term_ref,
    resid_ref,
    gain_ref,
    ids_ref,
    weights_ref,
    gate_hbm,
    up_hbm,
    down_hbm,
    out_ref,
    gate,
    up,
    down,
    table,
    mixed,
    normed,
    twin,
    chip_sum,
    sums,
    near,
    stage,
    piece,
    hidden,
    part,
    pair,
    finished,
    back,
    leave,
    last,
    ws,
    ms,
    mr,
    ts,
    tr,
    rs,
    rr,
    zs,
    zr,
    xs,
    xr,
    ps,
    pr,
    qs,
    qr,
    bs,
    br,
    ls,
    lr,
):
    place, turn = lax.axis_index("sp"), lax.axis_index("tp")
    chip, core = lax.div(turn, 2), lax.rem(turn, 2)
    other = 2 * chip + 1 - core
    rows, width = normed.shape
    slots = places * cap
    loads = [
        pltpu.make_async_copy(src, dst, ws.at[at])
        for at, (src, dst) in enumerate(((gate_hbm, gate), (up_hbm, up), (down_hbm, down)))
    ]
    for load in loads:
        load.start()
    table[0] = route_table(ids_ref[...], weights_ref[...], cap)
    greet_routes(places, chips)
    others = list(range(1, chips))

    def peer(apart):
        return 2 * flipped(chip, apart) + core

    def table_copy(apart):
        return remote(
            table.at[0], table.at[apart], ms.at[apart], mr.at[apart], tp=peer(apart)
        )

    def twin_copy(apart):
        spot = term_ref.at[flipped(chip, apart), 1 - core]
        return remote(spot, twin.at[apart], ts.at[apart], tr.at[apart], tp=other)

    def sum_copy(apart):
        return remote(
            chip_sum.at[apart], sums.at[apart], rs.at[apart], rr.at[apart], tp=peer(apart)
        )

    def near_copy(apart):
        return remote(normed, near.at[apart], zs.at[apart], zr.at[apart], tp=peer(apart))

    def route_copy(apart, away):
        expert = flipped(place, away)
        return remote(
            stage.at[apart, expert],
            piece.at[apart, core, place],
            xs.at[apart, away],
            xr.at[apart, away],
            sp=expert,
        )

    def pair_copy(apart):
        spot = piece.at[apart, core]
        return remote(spot, spot, ps.at[apart], pr.at[apart], tp=other)

    def part_copy(apart):
        return remote(
            part.at[apart, 1 - core], pair.at[apart], qs.at[apart], qr.at[apart], tp=other
        )

    def back_copy(apart, away):
        home = flipped(place, away)
        return remote(
            finished.at[apart, home],
            back.at[apart, place],
            bs.at[apart, away],
            br.at[apart, away],
            sp=home,
        )

    def last_copy(apart):
        return remote(leave.at[apart], last.at[apart], ls.at[apart], lr.at[apart], tp=peer(apart))

    turns = list(reversed(others)) + [0]
    for apart in turns:
        twin_copy(apart).start()
    for apart in others:
        table_copy(apart).start()
    total = resid_ref[...].astype(jnp.float32)
    for apart in turns:
        twin_copy(apart).wait_recv()
        both = term_ref[flipped(chip, apart), core].astype(jnp.float32)
        both = both + twin[apart].astype(jnp.float32)
        if apart:
            chip_sum[apart] = both.astype(jnp.bfloat16)
            sum_copy(apart).start()
        else:
            total = total + both
    for apart in others:
        sum_copy(apart).wait_recv()
        total = total + sums[apart].astype(jnp.float32)
    mixed[...] = total
    normed[...] = rms_scaled(total, gain_ref[...]).astype(jnp.bfloat16)
    for apart in others:
        near_copy(apart).start()

    slot = lax.broadcasted_iota(jnp.int32, (rows, slots), 1).astype(jnp.float32)

    def columns(apart):
        full = jnp.concatenate([table[apart], jnp.zeros((120, 128), jnp.float32)], axis=0)
        return full.T[0:rows, :]

    def send_out(apart):
        if apart:
            table_copy(apart).wait_recv()
            near_copy(apart).wait_recv()
        held = near[apart] if apart else normed[...]
        known = columns(apart)
        spread = jnp.zeros((rows, slots), jnp.float32)
        for which in range(2):
            spread = spread + jnp.where(slot == known[:, which : which + 1], 1.0, 0.0)
        sent = lax.dot_general(
            spread.astype(jnp.bfloat16),
            held,
            (((0,), (0,)), ((), ())),
            preferred_element_type=jnp.float32,
        )
        stage[apart] = sent.astype(jnp.bfloat16).reshape(places, cap, width)
        for away in reversed(range(1, places)):
            route_copy(apart, away).start()
        piece[apart, core, place] = stage[apart, place]

    def run_expert(apart):
        for away in range(1, places):
            route_copy(apart, away).wait_recv()
        pair_copy(apart).start()
        pair_copy(apart).wait_recv()
        tile = 256

        @pl.loop(0, hidden.shape[1] // tile)
        def _(step):
            cols = pl.ds(pl.multiple_of(step * tile, tile), tile)
            given = piece[apart].reshape(2 * slots, width)
            opened = jnp.dot(given, gate[:, cols], preferred_element_type=jnp.float32)
            raised = jnp.dot(given, up[:, cols], preferred_element_type=jnp.float32)
            hidden[:, cols] = (jax.nn.silu(opened) * raised).astype(jnp.bfloat16)

        wide = 512

        @pl.loop(0, width // wide)
        def _(step):
            cols = pl.ds(pl.multiple_of(step * wide, wide), wide)
            lowered = jnp.dot(hidden[...], down[:, cols], preferred_element_type=jnp.float32)
            part[apart, :, :, cols] = lowered.astype(jnp.bfloat16).reshape(2, slots, wide)

        part_copy(apart).start()

    def settle(apart):
        part_copy(apart).wait_recv()
        both = part[apart, core].astype(jnp.float32) + pair[apart].astype(jnp.float32)
        finished[apart] = both.astype(jnp.bfloat16).reshape(places, cap, width)
        if apart:
            send_back(apart)

    def send_back(apart):
        for away in reversed(range(1, places)):
            back_copy(apart, away).start()
        back[apart, place] = finished[apart, place]

    def gathered(apart):
        known = columns(apart)
        gather = jnp.zeros((rows, slots), jnp.float32)
        for which in range(2):
            own = known[:, which : which + 1]
            gather = gather + jnp.where(slot == own, known[:, which + 2 : which + 3], 0.0)
        high = gather.astype(jnp.bfloat16)
        low = (gather - high.astype(jnp.float32)).astype(jnp.bfloat16)
        for away in range(1, places):
            back_copy(apart, away).wait_recv()
        held = back[apart].reshape(slots, width)
        found = jnp.dot(high, held, preferred_element_type=jnp.float32)
        return found + jnp.dot(low, held, preferred_element_type=jnp.float32)

    ahead = min(3, chips)
    for apart in range(ahead):
        send_out(apart)
    for load in loads:
        load.wait()
    for apart in range(chips):
        run_expert(apart)
        if apart + ahead < chips:
            send_out(apart + ahead)
        if apart:
            settle(apart - 1)
    settle(chips - 1)
    send_back(0)
    for apart in others:
        leave[apart] = gathered(apart).astype(jnp.bfloat16)
        last_copy(apart).start()
    total = mixed[...] + gathered(0)
    for apart in others:
        last_copy(apart).wait_recv()
        total = total + last[apart].astype(jnp.float32)
    out_ref[...] = total.astype(jnp.bfloat16)
    for apart in range(chips):
        twin_copy(apart).wait_send()
        pair_copy(apart).wait_send()
        part_copy(apart).wait_send()
        if apart:
            table_copy(apart).wait_send()
            sum_copy(apart).wait_send()
            near_copy(apart).wait_send()
            last_copy(apart).wait_send()
        for away in range(1, places):
            route_copy(apart, away).wait_send()
            back_copy(apart, away).wait_send()


def vmem(count):
    return [pl.BlockSpec(memory_space=pltpu.VMEM)] * count


def routed_experts(
    term, resid, norm_gain, route_ids, route_weights, capacity, gate, upward, down
):
    places, chips = lax.axis_size("sp"), lax.axis_size("tp") // 2
    rows, width = resid.shape
    deep = gate.shape[2]
    slots = places * capacity
    sems = pltpu.SemaphoreType.DMA

    def held(*shape):
        return pltpu.VMEM(shape, jnp.bfloat16)

    return pl.pallas_call(
        functools.partial(experts_kernel, places, chips, capacity),
        out_shape=jax.ShapeDtypeStruct((rows, width), jnp.bfloat16),
        in_specs=vmem(5) + [pl.BlockSpec(memory_space=pl.ANY)] * 3,
        out_specs=vmem(1)[0],
        scratch_shapes=[
            held(width, deep),
            held(width, deep),
            held(deep, width),
            pltpu.VMEM((chips, 8, 128), jnp.float32),
            pltpu.VMEM((rows, width), jnp.float32),
            held(rows, width),
            held(chips, rows, width),
            held(chips, rows, width),
            held(chips, rows, width),
            held(chips, rows, width),
            held(chips, places, capacity, width),
            held(chips, 2, places, capacity, width),
            held(2 * slots, deep),
            held(chips, 2, slots, width),
            held(chips, slots, width),
            held(chips, places, capacity, width),
            held(chips, places, capacity, width),
            held(chips, rows, width),
            held(chips, rows, width),
            sems((3,)),
            *[sems((chips,))] * 8,
            *[sems((chips, places))] * 2,
            *[sems((chips,))] * 4,
            *[sems((chips, places))] * 2,
            *[sems((chips,))] * 2,
        ],
        compiler_params=pltpu.CompilerParams(
            collective_id=2, has_side_effects=True, vmem_limit_bytes=60 << 20
        ),
    )(
        term.reshape(chips, 2, rows, width),
        resid,
        norm_gain[None, :],
        route_ids,
        route_weights,
        gate[0],
        upward[0],
        down[0],
    )


def per_device(
    resid,
    query_a,
    key_a,
    value_a,
    query_b,
    key_b,
    value_b,
    mix_a,
    mix_b,
    head_gain_a,
    head_gain_b,
    proj_a,
    proj_b,
    norm_gain,
    route_ids,
    route_weights,
    expert_gate,
    expert_up,
    expert_down,
):
    sp_ways = lax.axis_size("sp")
    fits = query_a.shape[1] + query_b.shape[1] == sp_ways
    whole_b = query_b.shape[1] * query_b.shape[2] == query_a.shape[2]
    whole_b = whole_b and query_b.shape[2] == value_b.shape[2]
    fits = fits and query_a.shape[2] == value_a.shape[2] and whole_b
    attend = whole_heads if fits else zigzag_heads
    heads_out_a, heads_out_b = attend(
        query_a,
        key_a,
        value_a,
        query_b,
        key_b,
        value_b,
        mix_a,
        mix_b,
        head_gain_a,
        head_gain_b,
    )
    width = resid.shape[1]
    tok_rows = resid.shape[0]
    top_count = route_ids.shape[1]
    capacity = 3 * top_count * tok_rows // (2 * sp_ways)
    term = jnp.dot(heads_out_a, proj_a, preferred_element_type=jnp.float32)
    term = term + jnp.dot(heads_out_b, proj_b, preferred_element_type=jnp.float32)
    tp_ways = lax.axis_size("tp")
    paired = tp_ways % 2 == 0 and tp_ways & (tp_ways - 1) == 0 and sp_ways & (sp_ways - 1) == 0
    if paired and top_count == 2 and capacity % 16 == 0 and tok_rows <= 128:
        return routed_experts(
            term.astype(jnp.bfloat16),
            resid,
            norm_gain,
            route_ids,
            route_weights,
            capacity,
            expert_gate,
            expert_up,
            expert_down,
        )
    own_slots = slot_numbers(route_ids, sp_ways, capacity)
    mixed = resid.astype(jnp.float32) + lax.psum_scatter(
        lax.optimization_barrier(term.astype(jnp.bfloat16))
        .astype(jnp.float32)
        .astype(jnp.bfloat16),
        "tp",
        scatter_dimension=0,
        tiled=True,
    ).astype(jnp.float32)
    normed = rms_scaled(mixed, norm_gain).astype(jnp.bfloat16)
    lookup = jnp.arange(sp_ways * capacity, dtype=jnp.int32)[:, None]
    spread = jnp.zeros((sp_ways * capacity, tok_rows), jnp.float32)
    for which in range(top_count):
        spread = spread + (own_slots[:, which][None, :] == lookup).astype(jnp.float32)
    outgoing = jnp.dot(
        spread.astype(jnp.bfloat16), normed, preferred_element_type=jnp.float32
    ).astype(jnp.bfloat16)
    arrived = lax.all_to_all(
        outgoing.reshape(sp_ways, capacity, width), "sp", split_axis=0, concat_axis=0, tiled=True
    )
    piece = lax.all_gather(arrived.reshape(sp_ways * capacity, width), "tp", axis=0, tiled=True)
    gate = jnp.dot(piece, expert_gate[0], preferred_element_type=jnp.float32)
    upward = jnp.dot(piece, expert_up[0], preferred_element_type=jnp.float32)
    hidden = (jax.nn.silu(gate) * upward).astype(jnp.bfloat16)
    term = jnp.dot(hidden, expert_down[0], preferred_element_type=jnp.float32)
    summed = lax.psum_scatter(
        lax.optimization_barrier(term.astype(jnp.bfloat16))
        .astype(jnp.float32)
        .astype(jnp.bfloat16),
        "tp",
        scatter_dimension=0,
        tiled=True,
    )
    finished_rows = summed.reshape(sp_ways, capacity, width)
    back = lax.all_to_all(finished_rows, "sp", split_axis=0, concat_axis=0, tiled=True)
    picked = jnp.take(back.reshape(sp_ways * capacity, width), own_slots.reshape(-1), axis=0)
    picked = picked.reshape(tok_rows, top_count, width)
    output = mixed + jnp.sum(route_weights[:, :, None] * picked.astype(jnp.float32), axis=1)
    return output.astype(jnp.bfloat16)


def solution(mesh):
    placed = (
        P(("sp", "tp"), None),
        P("sp", "tp", None),
        P("sp", "tp", None),
        P("sp", "tp", None),
        P("sp", "tp", None),
        P("sp", "tp", None),
        P("sp", "tp", None),
        P("tp"),
        P("tp"),
        P(),
        P(),
        P("tp", None),
        P("tp", None),
        P(),
        P(("sp", "tp"), None),
        P(("sp", "tp"), None),
        P("sp", None, "tp"),
        P("sp", None, "tp"),
        P("sp", "tp", None),
    )
    return jax.shard_map(
        per_device, mesh=mesh, in_specs=placed, out_specs=P(("sp", "tp"), None), check_vma=False
    )
```

```python
import functools
import math

import jax
import jax.numpy as jnp
from jax import lax
from jax.experimental import pallas as pl
from jax.experimental.pallas import tpu as pltpu
from jax.sharding import PartitionSpec as P

EPS = 1e-06
NEG = -1e30
HEAD_SCALE = 1.0 - (0.8 - 0.6 * math.exp(-0.3))
KEY_STEP = 512


def partner(value, axis, apart):
    return lax.ppermute(value, axis, [(i, i ^ 1 << apart) for i in range(lax.axis_size(axis))])


def rms_scaled(values, gain):
    return values * lax.rsqrt(jnp.mean(values * values, axis=-1, keepdims=True) + EPS) * gain


def slot_numbers(route_rows, experts, capacity):
    count, top_count = route_rows.shape
    flat = route_rows.reshape(count * top_count)
    onehot = (flat[:, None] == jnp.arange(experts, dtype=jnp.int32)[None, :]).astype(jnp.int32)
    ranks = jnp.sum((jnp.cumsum(onehot, axis=0) - onehot) * onehot, axis=1)
    return (flat * capacity + ranks).reshape(count, top_count)


def empty_map(count, heads, width):
    return (
        jnp.zeros((count, heads, width), jnp.float32),
        jnp.full((heads, count), NEG, jnp.float32),
        jnp.zeros((heads, count), jnp.float32),
    )


def empty_group(query, value):
    return (
        empty_map(query.shape[0], query.shape[1], value.shape[2]),
        empty_map(query.shape[0], query.shape[1], value.shape[2]),
    )


def map_update(state, query, keys, values, allowed, scale):
    weighted, maximum, sums = state
    scores = jnp.einsum("qhd,khd->hqk", query, keys, preferred_element_type=jnp.float32) * scale
    scores = jnp.where(allowed[None], scores, NEG)
    fresh = jnp.maximum(maximum, jnp.max(scores, axis=2))
    weights = jnp.where(allowed[None], jnp.exp(scores - fresh[:, :, None]), 0.0)
    factor = jnp.exp(maximum - fresh)
    sums = sums * factor + jnp.sum(weights, axis=2)
    added = jnp.einsum(
        "hqk,khv->qhv", weights.astype(jnp.bfloat16), values, preferred_element_type=jnp.float32
    )
    weighted = weighted * jnp.transpose(factor)[:, :, None] + added
    return (weighted, fresh, sums)


def group_update(states, query, keys, values, allowed):
    width = query.shape[2] // 2
    scale = 1.0 / math.sqrt(width)
    return tuple(
        (
            map_update(
                states[which],
                query[:, :, which * width : (which + 1) * width],
                keys[:, :, which * width : (which + 1) * width],
                values,
                allowed,
                scale,
            )
            for which in range(2)
        )
    )


def set_update(carry, queries, pieces):
    rows_a, rows_b, query_pos = queries
    piece_key_a, piece_value_a, piece_key_b, piece_value_b = pieces
    length = piece_key_a.shape[0]
    step = math.gcd(length, KEY_STEP)
    latest = query_pos[-1]

    def inner(index, states):
        first = index * step

        def compute(current):
            keys_a = lax.dynamic_slice_in_dim(piece_key_a, first, step, 0)
            values_a = lax.dynamic_slice_in_dim(piece_value_a, first, step, 0)
            keys_b = lax.dynamic_slice_in_dim(piece_key_b, first, step, 0)
            values_b = lax.dynamic_slice_in_dim(piece_value_b, first, step, 0)
            key_pos = first + jnp.arange(step, dtype=jnp.int32)
            allowed = key_pos[None, :] <= query_pos[:, None]
            return (
                group_update(current[0], rows_a, keys_a, values_a, allowed),
                group_update(current[1], rows_b, keys_b, values_b, allowed),
            )

        return lax.cond(first <= latest, compute, lambda current: current, states)

    return lax.fori_loop(0, length // step, inner, carry)


def finish_group(states, mix, gain):
    outputs = [state[0] / jnp.transpose(state[2])[:, :, None] for state in states]
    mixed = outputs[0] - mix[None, :, None] * outputs[1]
    normed = rms_scaled(mixed, gain) * HEAD_SCALE
    return normed.astype(jnp.bfloat16).reshape(mixed.shape[0], -1)


def zigzag_heads(query_a, key_a, value_a, query_b, key_b, value_b, mix_a, mix_b, gain_a, gain_b):
    head_gain_a, head_gain_b = gain_a, gain_b
    seq_rows = query_a.shape[0]
    sp_ways = lax.axis_size("sp")
    place = lax.axis_index("sp")
    positions = place * seq_rows + jnp.arange(seq_rows, dtype=jnp.int32)
    levels = sp_ways.bit_length() - 1
    half = seq_rows // 2
    moved = jnp.concatenate(
        [query_a[half:].reshape(half, -1), query_b[half:].reshape(half, -1)], axis=1
    )
    for bit in range(levels):
        moved = partner(moved, "sp", bit)
    split_at = query_a.shape[1] * query_a.shape[2]
    far_a = moved[:, :split_at].reshape(half, query_a.shape[1], query_a.shape[2])
    far_b = moved[:, split_at:].reshape(half, query_b.shape[1], query_b.shape[2])
    far_pos = (sp_ways - 1 - place) * seq_rows + half + jnp.arange(half, dtype=jnp.int32)
    query_sets = ((query_a[:half], query_b[:half], positions[:half]), (far_a, far_b, far_pos))

    def fold_keys(carry, pieces):
        return tuple(
            (set_update(states, queries, pieces) for states, queries in zip(carry, query_sets))
        )

    initial = tuple(
        (
            (empty_group(queries[0], value_a), empty_group(queries[1], value_b))
            for queries in query_sets
        )
    )
    results = fold_keys(
        initial,
        (
            lax.all_gather(key_a, "sp", axis=0, tiled=True),
            lax.all_gather(value_a, "sp", axis=0, tiled=True),
            lax.all_gather(key_b, "sp", axis=0, tiled=True),
            lax.all_gather(value_b, "sp", axis=0, tiled=True),
        ),
    )
    finished = [
        (finish_group(states[0], mix_a, head_gain_a), finish_group(states[1], mix_b, head_gain_b))
        for states in results
    ]
    returned = jnp.concatenate([finished[1][0], finished[1][1]], axis=1)
    for bit in range(levels):
        returned = partner(returned, "sp", bit)
    width_a = finished[0][0].shape[1]
    heads_out_a = jnp.concatenate([finished[0][0], returned[:, :width_a]], axis=0)
    heads_out_b = jnp.concatenate([finished[0][1], returned[:, width_a:]], axis=0)
    return heads_out_a, heads_out_b


def remote(src, dst, send_sem, recv_sem, **where):
    return pltpu.make_async_remote_copy(
        src_ref=src,
        dst_ref=dst,
        send_sem=send_sem,
        recv_sem=recv_sem,
        device_id=where,
        device_id_type=pl.DeviceIdType.MESH,
    )


def greet_routes(places, chips):
    place, turn = lax.axis_index("sp"), lax.axis_index("tp")
    chip, core = lax.div(turn, 2), lax.rem(turn, 2)
    barrier = pltpu.get_barrier_semaphore()
    peers = [{"tp": 2 * chip + 1 - core}]
    peers += [{"tp": 2 * lax.rem(chip + apart, chips) + core} for apart in range(1, chips)]
    peers += [{"sp": lax.rem(place + apart, places)} for apart in range(1, places)]
    for peer in peers:
        pl.semaphore_signal(
            barrier, inc=1, device_id=peer, device_id_type=pl.DeviceIdType.MESH
        )
    pl.semaphore_wait(barrier, len(peers))


def flipped(value, apart):
    bit = 1
    while bit <= apart:
        if apart & bit:
            value = value + bit - 2 * bit * lax.rem(lax.div(value, bit), 2)
        bit *= 2
    return value


def route_table(ids, weights, cap):
    rows = ids.shape[1]
    joined = [ids.astype(jnp.float32), weights, jnp.zeros((4, rows), jnp.float32)]
    full = jnp.concatenate(joined, axis=0)
    if rows < 128:
        full = jnp.concatenate([full, jnp.zeros((8, 128 - rows), jnp.float32)], axis=1)
    full = full.T[0:rows, :]
    ids, weights = full[:, 0:2].astype(jnp.int32), full[:, 2:4]
    lane = lax.broadcasted_iota(jnp.int32, (rows, 128), 1)
    hits = [ids[:, which : which + 1] == lane for which in range(2)]
    named = jnp.where(hits[0], 1.0, 0.0) + jnp.where(hits[1], 1.0, 0.0)
    above = lax.broadcasted_iota(jnp.int32, (rows, rows), 0)
    above = above > lax.broadcasted_iota(jnp.int32, (rows, rows), 1)
    ranks = jnp.dot(
        jnp.where(above, 1.0, 0.0).astype(jnp.bfloat16),
        named.astype(jnp.bfloat16),
        preferred_element_type=jnp.float32,
    )
    spots = ranks + (lane * cap).astype(jnp.float32)
    table = jnp.zeros((rows, 128), jnp.float32)
    for which in range(2):
        spot = jnp.sum(jnp.where(hits[which], spots, 0.0), axis=1, keepdims=True)
        table = jnp.where(lane == which, spot, table)
        table = jnp.where(lane == which + 2, weights[:, which : which + 1], table)
    table = jnp.concatenate([table, jnp.zeros((128 - rows, 128), jnp.float32)], axis=0)
    return table.T[0:8, :]


def head_units(heads_a, heads_b):
    half = heads_a // 2
    order = [("a", head) for head in range(half)]
    order += [("b", head) for head in range(heads_b)]
    return order + [("a", head) for head in range(half, heads_a)]


def chosen(me, units, for_a, for_b):
    value = for_b(units[0][1]) if units[0][0] == "b" else for_a(units[0][1])
    for at, (group, head) in enumerate(units):
        if at:
            value = jnp.where(me == at, for_a(head) if group == "a" else for_b(head), value)
    return value


def column(row):
    return jnp.broadcast_to(row, (8, row.shape[1])).T[:, 0:1]


def attend_block(chunk, block, queries, keys, values_t, heads, facts):
    pick, scale, mix, gain, valid, share = facts
    rows = queries.shape[1]
    key = lax.broadcasted_iota(jnp.int32, (chunk, 2 * chunk), 0)
    asks = lax.broadcasted_iota(jnp.int32, (chunk, 2 * chunk), 1)
    allowed = key <= jnp.where(asks >= chunk, asks - chunk, asks)
    for part in reversed(range(rows // chunk)):
        first = part * chunk
        before = block * rows + first
        length = before + chunk
        query = queries[block, first : first + chunk, :]
        picked = jnp.concatenate([query * pick[0], query * pick[1]], axis=0)
        scores = lax.dot_general(
            keys[0:length, :],
            picked,
            (((1,), (1,)), ((), ())),
            preferred_element_type=jnp.float32,
        )
        newest = jnp.where(allowed, scores[before:], NEG)
        if before:
            scores = jnp.concatenate([scores[:before], newest], axis=0)
        else:
            scores = newest
        top = jnp.max(scores, axis=0, keepdims=True)
        weights = jnp.exp2((scores - top) * scale)
        sums = jnp.sum(weights, axis=0, keepdims=True)
        found = jnp.dot(
            values_t[:, 0:length], weights.astype(jnp.bfloat16), preferred_element_type=jnp.float32
        )
        found = found / sums
        mixed = found[:, :chunk] - mix * found[:, chunk:]
        square = jnp.sum(mixed * mixed * valid, axis=0, keepdims=True) * share
        heads[block, :, first : first + chunk] = (
            mixed * lax.rsqrt(square + EPS) * gain * HEAD_SCALE
        ).astype(jnp.bfloat16)


def layer_kernel(
    places,
    chips,
    cap,
    units,
    qa_ref,
    ka_ref,
    va_ref,
    qb_ref,
    kb_ref,
    vb_ref,
    mix_a_ref,
    mix_b_ref,
    gain_a_ref,
    gain_b_ref,
    resid_ref,
    gain_ref,
    ids_ref,
    weights_ref,
    proj_a_hbm,
    proj_b_hbm,
    gate_hbm,
    up_hbm,
    down_hbm,
    out_ref,
    ready_a,
    ready_b,
    got,
    keys,
    values_t,
    heads,
    joined,
    turned,
    proj,
    gate,
    up,
    down,
    term,
    table,
    mixed,
    normed,
    twin,
    chip_sum,
    sums,
    near,
    stage,
    piece,
    hidden,
    part,
    pair,
    finished,
    back,
    leave,
    last,
    ins,
    inr,
    outs,
    outr,
    ws,
    ms,
    mr,
    ts,
    tr,
    rs,
    rr,
    zs,
    zr,
    xs,
    xr,
    ps,
    pr,
    qs,
    qr,
    bs,
    br,
    ls,
    lr,
):
    place, turn = lax.axis_index("sp"), lax.axis_index("tp")
    chip, core = lax.div(turn, 2), lax.rem(turn, 2)
    other = 2 * chip + 1 - core
    rows, width = normed.shape
    slots = places * cap
    depth_a = proj_a_hbm.shape[0]
    pairs = (
        (proj_a_hbm, proj.at[0:depth_a]),
        (proj_b_hbm, proj.at[depth_a : proj.shape[0]]),
        (gate_hbm, gate),
        (up_hbm, up),
        (down_hbm, down),
    )
    loads = [pltpu.make_async_copy(src, dst, ws.at[at]) for at, (src, dst) in enumerate(pairs)]
    for load in loads:
        load.start()

    seq, wide = qa_ref.shape[0], qa_ref.shape[2]
    narrow = qb_ref.shape[2]
    half = seq // 2
    for at, ref in enumerate((qa_ref, ka_ref, va_ref)):
        split = pltpu.einshape("abc->bac", ref[...])
        for head in range(split.shape[0]):
            ready_a[head, at * seq : (at + 1) * seq, :] = split[head]
    asked, known, valued = [
        pltpu.einshape("abc->bac", ref[...]) for ref in (qb_ref, kb_ref, vb_ref)
    ]
    for head in range(asked.shape[0]):
        ready_b[head, 0:seq, :] = jnp.concatenate([asked[head], known[head]], axis=1)
        ready_b[head, seq : seq + half, :] = jnp.concatenate(
            [valued[head][:half], valued[head][half:]], axis=1
        )
    table[0] = route_table(ids_ref[...], weights_ref[...], cap)
    greet_routes(places, chips)

    sizes = [3 * seq if group == "a" else seq + half for group, _ in units]
    spans, reach = [], {"a": 0, "b": depth_a}
    for group, head in units:
        tall = wide if group == "a" else narrow
        spans.append((reach[group] + head * tall, tall))

    def unit_ready(unit):
        group, head = units[unit]
        return (ready_a if group == "a" else ready_b).at[head]

    def in_copy(unit, sender, away):
        return remote(
            unit_ready(unit),
            got.at[sender, 0 : sizes[unit]],
            ins.at[away],
            inr.at[sender],
            sp=unit,
        )

    def out_copy(unit, block):
        start, tall = spans[unit]
        return remote(
            heads.at[block, 0:tall],
            joined.at[start : start + tall],
            outs.at[block],
            outr.at[unit],
            sp=block,
        )

    for away in reversed(range(1, places)):
        for unit in range(places):

            @pl.when(place == unit ^ away)
            def _():
                in_copy(unit, place, away).start()

    def settle_block(sender, unit, held):
        span = slice(sender * seq, (sender + 1) * seq)
        if units[unit][0] == "a":
            keys[span, :] = held[seq : 2 * seq, :]
            values_t[:, span] = held[2 * seq : 3 * seq, :].T
        else:
            both = held[0:seq, :].astype(jnp.float32)
            keys[span, :] = pltpu.roll(both, narrow, 1).astype(jnp.bfloat16)
            packed = held[seq : seq + half, :].astype(jnp.float32).T
            values_t[0:narrow, sender * seq : sender * seq + half] = packed[:narrow].astype(
                jnp.bfloat16
            )
            values_t[0:narrow, sender * seq + half : (sender + 1) * seq] = packed[
                narrow:
            ].astype(jnp.bfloat16)
            values_t[narrow:wide, span] = jnp.zeros((wide - narrow, seq), jnp.bfloat16)

    for unit in range(places):

        @pl.when(place == unit)
        def _():
            mine = unit_ready(unit)
            got[unit, 0:seq] = mine[0:seq, :]
            settle_block(unit, unit, mine)
            for away in reversed(range(1, places)):
                sender = unit ^ away
                in_copy(unit, sender, away).wait_recv()
                settle_block(sender, unit, got.at[sender])

    is_a = chosen(place, units, lambda head: 1, lambda head: 0) == 1
    lane = lax.broadcasted_iota(jnp.int32, (1, wide), 1)
    map_wide = jnp.where(is_a, wide // 2, narrow // 2)
    pick = []
    for which in range(2):
        inside = (lane >= which * map_wide) & (lane < (which + 1) * map_wide)
        pick.append(jnp.where(inside, 1.0, 0.0).astype(jnp.bfloat16))
    scale = jnp.where(
        is_a,
        math.log2(math.e) / math.sqrt(wide // 2),
        math.log2(math.e) / math.sqrt(narrow // 2),
    )
    share = jnp.where(is_a, 1.0 / wide, 1.0 / narrow)
    mix = chosen(place, units, lambda head: mix_a_ref[head], lambda head: mix_b_ref[head])
    padded = jnp.concatenate(
        [gain_b_ref[...], jnp.zeros((1, wide - narrow), jnp.float32)], axis=1
    )
    gain = column(jnp.where(is_a, gain_a_ref[...], padded))
    valid = column(jnp.where(lane < jnp.where(is_a, wide, narrow), 1.0, 0.0))
    facts = (pick, scale, mix, gain, valid, share)
    chunk = math.gcd(seq, 256)
    queries = got.at[:, 0:seq]
    for block in reversed(range(places)):
        attend_block(chunk, block, queries, keys, values_t, heads, facts)
        for unit in range(places):

            @pl.when(place == unit)
            def _():
                if unit == block:
                    start, tall = spans[unit]
                    joined[start : start + tall, :] = heads[block, 0:tall, :]
                else:
                    out_copy(unit, block).start()

    others = list(range(1, chips))

    def peer(apart):
        return 2 * flipped(chip, apart) + core

    def table_copy(apart):
        return remote(
            table.at[0], table.at[apart], ms.at[apart], mr.at[apart], tp=peer(apart)
        )

    def twin_copy(apart):
        spot = term.at[apart, 1 - core]
        return remote(spot, twin.at[apart], ts.at[apart], tr.at[apart], tp=other)

    def sum_copy(apart):
        return remote(
            chip_sum.at[apart], sums.at[apart], rs.at[apart], rr.at[apart], tp=peer(apart)
        )

    def near_copy(apart):
        return remote(normed, near.at[apart], zs.at[apart], zr.at[apart], tp=peer(apart))

    def route_copy(apart, away):
        expert = flipped(place, away)
        return remote(
            stage.at[apart, expert],
            piece.at[apart, core, place],
            xs.at[apart, away],
            xr.at[apart, away],
            sp=expert,
        )

    def pair_copy(apart):
        spot = piece.at[apart, core]
        return remote(spot, spot, ps.at[apart], pr.at[apart], tp=other)

    def part_copy(apart):
        return remote(
            part.at[apart, 1 - core], pair.at[apart], qs.at[apart], qr.at[apart], tp=other
        )

    def back_copy(apart, away):
        home = flipped(place, away)
        return remote(
            finished.at[apart, home],
            back.at[apart, place],
            bs.at[apart, away],
            br.at[apart, away],
            sp=home,
        )

    def last_copy(apart):
        return remote(leave.at[apart], last.at[apart], ls.at[apart], lr.at[apart], tp=peer(apart))

    for apart in others:
        table_copy(apart).start()
    for unit in range(places):

        @pl.when(place != unit)
        def _():
            out_copy(unit, unit).wait_recv()

    for load in loads[:2]:
        load.wait()
    turned[...] = joined[...].T
    turns = list(reversed(others)) + [0]
    for apart in turns:
        first = pl.multiple_of(flipped(chip, apart) * (2 * rows), 2 * rows)
        given = turned[pl.ds(first, 2 * rows), :]
        summed = jnp.dot(given, proj[...], preferred_element_type=jnp.float32)
        term[apart] = summed.astype(jnp.bfloat16).reshape(2, rows, width)
        twin_copy(apart).start()
    total = resid_ref[...].astype(jnp.float32)
    for apart in turns:
        twin_copy(apart).wait_recv()
        both = term[apart, core].astype(jnp.float32) + twin[apart].astype(jnp.float32)
        if apart:
            chip_sum[apart] = both.astype(jnp.bfloat16)
            sum_copy(apart).start()
        else:
            total = total + both
    for apart in others:
        sum_copy(apart).wait_recv()
        total = total + sums[apart].astype(jnp.float32)
    mixed[...] = total
    normed[...] = rms_scaled(total, gain_ref[...]).astype(jnp.bfloat16)
    for apart in others:
        near_copy(apart).start()

    slot = lax.broadcasted_iota(jnp.int32, (rows, slots), 1).astype(jnp.float32)

    def columns(apart):
        full = jnp.concatenate([table[apart], jnp.zeros((120, 128), jnp.float32)], axis=0)
        return full.T[0:rows, :]

    def send_out(apart):
        if apart:
            table_copy(apart).wait_recv()
            near_copy(apart).wait_recv()
        held = near[apart] if apart else normed[...]
        known = columns(apart)
        spread = jnp.zeros((rows, slots), jnp.float32)
        for which in range(2):
            spread = spread + jnp.where(slot == known[:, which : which + 1], 1.0, 0.0)
        sent = lax.dot_general(
            spread.astype(jnp.bfloat16),
            held,
            (((0,), (0,)), ((), ())),
            preferred_element_type=jnp.float32,
        )
        stage[apart] = sent.astype(jnp.bfloat16).reshape(places, cap, width)
        for away in reversed(range(1, places)):
            route_copy(apart, away).start()
        piece[apart, core, place] = stage[apart, place]

    def run_expert(apart):
        for away in range(1, places):
            route_copy(apart, away).wait_recv()
        pair_copy(apart).start()
        pair_copy(apart).wait_recv()
        tile = 256

        @pl.loop(0, hidden.shape[1] // tile)
        def _(step):
            cols = pl.ds(pl.multiple_of(step * tile, tile), tile)
            given = piece[apart].reshape(2 * slots, width)
            opened = jnp.dot(given, gate[:, cols], preferred_element_type=jnp.float32)
            raised = jnp.dot(given, up[:, cols], preferred_element_type=jnp.float32)
            hidden[:, cols] = (jax.nn.silu(opened) * raised).astype(jnp.bfloat16)

        wide = 512

        @pl.loop(0, width // wide)
        def _(step):
            cols = pl.ds(pl.multiple_of(step * wide, wide), wide)
            lowered = jnp.dot(hidden[...], down[:, cols], preferred_element_type=jnp.float32)
            part[apart, :, :, cols] = lowered.astype(jnp.bfloat16).reshape(2, slots, wide)

        part_copy(apart).start()

    def settle(apart):
        part_copy(apart).wait_recv()
        both = part[apart, core].astype(jnp.float32) + pair[apart].astype(jnp.float32)
        finished[apart] = both.astype(jnp.bfloat16).reshape(places, cap, width)
        if apart:
            send_back(apart)

    def send_back(apart):
        for away in reversed(range(1, places)):
            back_copy(apart, away).start()
        back[apart, place] = finished[apart, place]

    def gathered(apart):
        known = columns(apart)
        gather = jnp.zeros((rows, slots), jnp.float32)
        for which in range(2):
            own = known[:, which : which + 1]
            gather = gather + jnp.where(slot == own, known[:, which + 2 : which + 3], 0.0)
        high = gather.astype(jnp.bfloat16)
        low = (gather - high.astype(jnp.float32)).astype(jnp.bfloat16)
        for away in range(1, places):
            back_copy(apart, away).wait_recv()
        held = back[apart].reshape(slots, width)
        found = jnp.dot(high, held, preferred_element_type=jnp.float32)
        return found + jnp.dot(low, held, preferred_element_type=jnp.float32)

    ahead = min(3, chips)
    for apart in range(ahead):
        send_out(apart)
    for load in loads[2:]:
        load.wait()
    for apart in range(chips):
        run_expert(apart)
        if apart + ahead < chips:
            send_out(apart + ahead)
        if apart:
            settle(apart - 1)
    settle(chips - 1)
    send_back(0)
    for apart in others:
        leave[apart] = gathered(apart).astype(jnp.bfloat16)
        last_copy(apart).start()
    total = mixed[...] + gathered(0)
    for apart in others:
        last_copy(apart).wait_recv()
        total = total + last[apart].astype(jnp.float32)
    out_ref[...] = total.astype(jnp.bfloat16)
    for unit in range(places):

        @pl.when(place == unit)
        def _():
            for away in range(1, places):
                in_copy(unit ^ away, unit, away).wait_send()
                out_copy(unit, unit ^ away).wait_send()

    for apart in range(chips):
        twin_copy(apart).wait_send()
        pair_copy(apart).wait_send()
        part_copy(apart).wait_send()
        if apart:
            table_copy(apart).wait_send()
            sum_copy(apart).wait_send()
            near_copy(apart).wait_send()
            last_copy(apart).wait_send()
        for away in range(1, places):
            route_copy(apart, away).wait_send()
            back_copy(apart, away).wait_send()


def vmem(count):
    return [pl.BlockSpec(memory_space=pltpu.VMEM)] * count


def whole_layer(attention, resid, norm_gain, ids, weights, capacity, proj, experts):
    query_a, key_a, value_a, query_b, key_b, value_b, mix_a, mix_b, gain_a, gain_b = attention
    places, chips = lax.axis_size("sp"), lax.axis_size("tp") // 2
    rows, width = resid.shape
    seq, heads_a, wide = query_a.shape
    heads_b, narrow = query_b.shape[1:]
    deep = experts[0].shape[2]
    slots = places * capacity
    tall = proj[0].shape[0] + proj[1].shape[0]
    sems = pltpu.SemaphoreType.DMA
    units = head_units(heads_a, heads_b)

    def held(*shape):
        return pltpu.VMEM(shape, jnp.bfloat16)

    smem = [pl.BlockSpec(memory_space=pltpu.SMEM)] * 2
    return pl.pallas_call(
        functools.partial(layer_kernel, places, chips, capacity, units),
        out_shape=jax.ShapeDtypeStruct((rows, width), jnp.bfloat16),
        in_specs=vmem(6) + smem + vmem(6) + [pl.BlockSpec(memory_space=pl.ANY)] * 5,
        out_specs=vmem(1)[0],
        scratch_shapes=[
            held(heads_a, 3 * seq, wide),
            held(heads_b, seq + seq // 2, wide),
            held(places, 3 * seq, wide),
            held(places * seq, wide),
            held(wide, places * seq),
            held(places, wide, seq),
            held(tall, seq),
            held(seq, tall),
            held(tall, width),
            held(width, deep),
            held(width, deep),
            held(deep, width),
            held(chips, 2, rows, width),
            pltpu.VMEM((chips, 8, 128), jnp.float32),
            pltpu.VMEM((rows, width), jnp.float32),
            held(rows, width),
            held(chips, rows, width),
            held(chips, rows, width),
            held(chips, rows, width),
            held(chips, rows, width),
            held(chips, places, capacity, width),
            held(chips, 2, places, capacity, width),
            held(2 * slots, deep),
            held(chips, 2, slots, width),
            held(chips, slots, width),
            held(chips, places, capacity, width),
            held(chips, places, capacity, width),
            held(chips, rows, width),
            held(chips, rows, width),
            *[sems((places,))] * 4,
            sems((5,)),
            *[sems((chips,))] * 8,
            *[sems((chips, places))] * 2,
            *[sems((chips,))] * 4,
            *[sems((chips, places))] * 2,
            *[sems((chips,))] * 2,
        ],
        compiler_params=pltpu.CompilerParams(
            collective_id=1, has_side_effects=True, vmem_limit_bytes=67043328
        ),
    )(
        query_a,
        key_a,
        value_a,
        query_b,
        key_b,
        value_b,
        mix_a,
        mix_b,
        gain_a[None, :],
        gain_b[None, :],
        resid,
        norm_gain[None, :],
        ids.T,
        weights.T,
        *proj,
        *[expert[0] for expert in experts],
    )


def per_device(
    resid,
    query_a,
    key_a,
    value_a,
    query_b,
    key_b,
    value_b,
    mix_a,
    mix_b,
    head_gain_a,
    head_gain_b,
    proj_a,
    proj_b,
    norm_gain,
    route_ids,
    route_weights,
    expert_gate,
    expert_up,
    expert_down,
):
    sp_ways, tp_ways = lax.axis_size("sp"), lax.axis_size("tp")
    width = resid.shape[1]
    tok_rows = resid.shape[0]
    top_count = route_ids.shape[1]
    capacity = 3 * top_count * tok_rows // (2 * sp_ways)
    attention = (
        query_a,
        key_a,
        value_a,
        query_b,
        key_b,
        value_b,
        mix_a,
        mix_b,
        head_gain_a,
        head_gain_b,
    )
    wide, narrow = query_a.shape[2], query_b.shape[2]
    fits = query_a.shape[1] + query_b.shape[1] == sp_ways and wide == 128 == 2 * narrow
    fits = fits and wide == value_a.shape[2] and narrow == value_b.shape[2]
    paired = tp_ways % 2 == 0 and tp_ways & (tp_ways - 1) == 0 and sp_ways & (sp_ways - 1) == 0
    paired = paired and top_count == 2 and capacity % 16 == 0 and tok_rows <= 128
    if fits and paired:
        return whole_layer(
            attention,
            resid,
            norm_gain,
            route_ids,
            route_weights,
            capacity,
            (proj_a, proj_b),
            (expert_gate, expert_up, expert_down),
        )
    heads_out_a, heads_out_b = zigzag_heads(*attention)
    term = jnp.dot(heads_out_a, proj_a, preferred_element_type=jnp.float32)
    term = term + jnp.dot(heads_out_b, proj_b, preferred_element_type=jnp.float32)
    own_slots = slot_numbers(route_ids, sp_ways, capacity)
    mixed = resid.astype(jnp.float32) + lax.psum_scatter(
        lax.optimization_barrier(term.astype(jnp.bfloat16))
        .astype(jnp.float32)
        .astype(jnp.bfloat16),
        "tp",
        scatter_dimension=0,
        tiled=True,
    ).astype(jnp.float32)
    normed = rms_scaled(mixed, norm_gain).astype(jnp.bfloat16)
    lookup = jnp.arange(sp_ways * capacity, dtype=jnp.int32)[:, None]
    spread = jnp.zeros((sp_ways * capacity, tok_rows), jnp.float32)
    for which in range(top_count):
        spread = spread + (own_slots[:, which][None, :] == lookup).astype(jnp.float32)
    outgoing = jnp.dot(
        spread.astype(jnp.bfloat16), normed, preferred_element_type=jnp.float32
    ).astype(jnp.bfloat16)
    arrived = lax.all_to_all(
        outgoing.reshape(sp_ways, capacity, width), "sp", split_axis=0, concat_axis=0, tiled=True
    )
    piece = lax.all_gather(arrived.reshape(sp_ways * capacity, width), "tp", axis=0, tiled=True)
    gate = jnp.dot(piece, expert_gate[0], preferred_element_type=jnp.float32)
    upward = jnp.dot(piece, expert_up[0], preferred_element_type=jnp.float32)
    hidden = (jax.nn.silu(gate) * upward).astype(jnp.bfloat16)
    term = jnp.dot(hidden, expert_down[0], preferred_element_type=jnp.float32)
    summed = lax.psum_scatter(
        lax.optimization_barrier(term.astype(jnp.bfloat16))
        .astype(jnp.float32)
        .astype(jnp.bfloat16),
        "tp",
        scatter_dimension=0,
        tiled=True,
    )
    finished_rows = summed.reshape(sp_ways, capacity, width)
    back = lax.all_to_all(finished_rows, "sp", split_axis=0, concat_axis=0, tiled=True)
    picked = jnp.take(back.reshape(sp_ways * capacity, width), own_slots.reshape(-1), axis=0)
    picked = picked.reshape(tok_rows, top_count, width)
    output = mixed + jnp.sum(route_weights[:, :, None] * picked.astype(jnp.float32), axis=1)
    return output.astype(jnp.bfloat16)


def solution(mesh):
    placed = (
        P(("sp", "tp"), None),
        P("sp", "tp", None),
        P("sp", "tp", None),
        P("sp", "tp", None),
        P("sp", "tp", None),
        P("sp", "tp", None),
        P("sp", "tp", None),
        P("tp"),
        P("tp"),
        P(),
        P(),
        P("tp", None),
        P("tp", None),
        P(),
        P(("sp", "tp"), None),
        P(("sp", "tp"), None),
        P("sp", None, "tp"),
        P("sp", None, "tp"),
        P("sp", "tp", None),
    )
    return jax.shard_map(
        per_device, mesh=mesh, in_specs=placed, out_specs=P(("sp", "tp"), None), check_vma=False
    )
```

```python
import functools
import math

import jax
import jax.numpy as jnp
from jax import lax
from jax.experimental import pallas as pl
from jax.experimental.pallas import tpu as pltpu
from jax.sharding import PartitionSpec as P

EPS = 1e-06
NEG = -1e30
HEAD_SCALE = 1.0 - (0.8 - 0.6 * math.exp(-0.3))
KEY_STEP = 512


def partner(value, axis, apart):
    return lax.ppermute(value, axis, [(i, i ^ 1 << apart) for i in range(lax.axis_size(axis))])


def rms_scaled(values, gain):
    return values * lax.rsqrt(jnp.mean(values * values, axis=-1, keepdims=True) + EPS) * gain


def slot_numbers(route_rows, experts, capacity):
    count, top_count = route_rows.shape
    flat = route_rows.reshape(count * top_count)
    onehot = (flat[:, None] == jnp.arange(experts, dtype=jnp.int32)[None, :]).astype(jnp.int32)
    ranks = jnp.sum((jnp.cumsum(onehot, axis=0) - onehot) * onehot, axis=1)
    return (flat * capacity + ranks).reshape(count, top_count)


def empty_map(count, heads, width):
    return (
        jnp.zeros((count, heads, width), jnp.float32),
        jnp.full((heads, count), NEG, jnp.float32),
        jnp.zeros((heads, count), jnp.float32),
    )


def empty_group(query, value):
    return (
        empty_map(query.shape[0], query.shape[1], value.shape[2]),
        empty_map(query.shape[0], query.shape[1], value.shape[2]),
    )


def map_update(state, query, keys, values, allowed, scale):
    weighted, maximum, sums = state
    scores = jnp.einsum("qhd,khd->hqk", query, keys, preferred_element_type=jnp.float32) * scale
    scores = jnp.where(allowed[None], scores, NEG)
    fresh = jnp.maximum(maximum, jnp.max(scores, axis=2))
    weights = jnp.where(allowed[None], jnp.exp(scores - fresh[:, :, None]), 0.0)
    factor = jnp.exp(maximum - fresh)
    sums = sums * factor + jnp.sum(weights, axis=2)
    added = jnp.einsum(
        "hqk,khv->qhv", weights.astype(jnp.bfloat16), values, preferred_element_type=jnp.float32
    )
    weighted = weighted * jnp.transpose(factor)[:, :, None] + added
    return (weighted, fresh, sums)


def group_update(states, query, keys, values, allowed):
    width = query.shape[2] // 2
    scale = 1.0 / math.sqrt(width)
    return tuple(
        (
            map_update(
                states[which],
                query[:, :, which * width : (which + 1) * width],
                keys[:, :, which * width : (which + 1) * width],
                values,
                allowed,
                scale,
            )
            for which in range(2)
        )
    )


def set_update(carry, queries, pieces):
    rows_a, rows_b, query_pos = queries
    piece_key_a, piece_value_a, piece_key_b, piece_value_b = pieces
    length = piece_key_a.shape[0]
    step = math.gcd(length, KEY_STEP)
    latest = query_pos[-1]

    def inner(index, states):
        first = index * step

        def compute(current):
            keys_a = lax.dynamic_slice_in_dim(piece_key_a, first, step, 0)
            values_a = lax.dynamic_slice_in_dim(piece_value_a, first, step, 0)
            keys_b = lax.dynamic_slice_in_dim(piece_key_b, first, step, 0)
            values_b = lax.dynamic_slice_in_dim(piece_value_b, first, step, 0)
            key_pos = first + jnp.arange(step, dtype=jnp.int32)
            allowed = key_pos[None, :] <= query_pos[:, None]
            return (
                group_update(current[0], rows_a, keys_a, values_a, allowed),
                group_update(current[1], rows_b, keys_b, values_b, allowed),
            )

        return lax.cond(first <= latest, compute, lambda current: current, states)

    return lax.fori_loop(0, length // step, inner, carry)


def finish_group(states, mix, gain):
    outputs = [state[0] / jnp.transpose(state[2])[:, :, None] for state in states]
    mixed = outputs[0] - mix[None, :, None] * outputs[1]
    normed = rms_scaled(mixed, gain) * HEAD_SCALE
    return normed.astype(jnp.bfloat16).reshape(mixed.shape[0], -1)


def zigzag_heads(query_a, key_a, value_a, query_b, key_b, value_b, mix_a, mix_b, gain_a, gain_b):
    head_gain_a, head_gain_b = gain_a, gain_b
    seq_rows = query_a.shape[0]
    sp_ways = lax.axis_size("sp")
    place = lax.axis_index("sp")
    positions = place * seq_rows + jnp.arange(seq_rows, dtype=jnp.int32)
    levels = sp_ways.bit_length() - 1
    half = seq_rows // 2
    moved = jnp.concatenate(
        [query_a[half:].reshape(half, -1), query_b[half:].reshape(half, -1)], axis=1
    )
    for bit in range(levels):
        moved = partner(moved, "sp", bit)
    split_at = query_a.shape[1] * query_a.shape[2]
    far_a = moved[:, :split_at].reshape(half, query_a.shape[1], query_a.shape[2])
    far_b = moved[:, split_at:].reshape(half, query_b.shape[1], query_b.shape[2])
    far_pos = (sp_ways - 1 - place) * seq_rows + half + jnp.arange(half, dtype=jnp.int32)
    query_sets = ((query_a[:half], query_b[:half], positions[:half]), (far_a, far_b, far_pos))

    def fold_keys(carry, pieces):
        return tuple(
            (set_update(states, queries, pieces) for states, queries in zip(carry, query_sets))
        )

    initial = tuple(
        (
            (empty_group(queries[0], value_a), empty_group(queries[1], value_b))
            for queries in query_sets
        )
    )
    results = fold_keys(
        initial,
        (
            lax.all_gather(key_a, "sp", axis=0, tiled=True),
            lax.all_gather(value_a, "sp", axis=0, tiled=True),
            lax.all_gather(key_b, "sp", axis=0, tiled=True),
            lax.all_gather(value_b, "sp", axis=0, tiled=True),
        ),
    )
    finished = [
        (finish_group(states[0], mix_a, head_gain_a), finish_group(states[1], mix_b, head_gain_b))
        for states in results
    ]
    returned = jnp.concatenate([finished[1][0], finished[1][1]], axis=1)
    for bit in range(levels):
        returned = partner(returned, "sp", bit)
    width_a = finished[0][0].shape[1]
    heads_out_a = jnp.concatenate([finished[0][0], returned[:, :width_a]], axis=0)
    heads_out_b = jnp.concatenate([finished[0][1], returned[:, width_a:]], axis=0)
    return heads_out_a, heads_out_b


def remote(src, dst, send_sem, recv_sem, **where):
    return pltpu.make_async_remote_copy(
        src_ref=src,
        dst_ref=dst,
        send_sem=send_sem,
        recv_sem=recv_sem,
        device_id=where,
        device_id_type=pl.DeviceIdType.MESH,
    )


def greet_routes(places, chips):
    place, turn = lax.axis_index("sp"), lax.axis_index("tp")
    chip, core = lax.div(turn, 2), lax.rem(turn, 2)
    barrier = pltpu.get_barrier_semaphore()
    peers = [{"tp": 2 * chip + 1 - core}]
    peers += [{"tp": 2 * lax.rem(chip + apart, chips) + core} for apart in range(1, chips)]
    peers += [{"sp": lax.rem(place + apart, places)} for apart in range(1, places)]
    for peer in peers:
        pl.semaphore_signal(
            barrier, inc=1, device_id=peer, device_id_type=pl.DeviceIdType.MESH
        )
    pl.semaphore_wait(barrier, len(peers))


def flipped(value, apart):
    bit = 1
    while bit <= apart:
        if apart & bit:
            value = value + bit - 2 * bit * lax.rem(lax.div(value, bit), 2)
        bit *= 2
    return value


def route_table(ids, weights, cap):
    rows = ids.shape[1]
    joined = [ids.astype(jnp.float32), weights, jnp.zeros((4, rows), jnp.float32)]
    full = jnp.concatenate(joined, axis=0)
    if rows < 128:
        full = jnp.concatenate([full, jnp.zeros((8, 128 - rows), jnp.float32)], axis=1)
    full = full.T[0:rows, :]
    ids, weights = full[:, 0:2].astype(jnp.int32), full[:, 2:4]
    lane = lax.broadcasted_iota(jnp.int32, (rows, 128), 1)
    hits = [ids[:, which : which + 1] == lane for which in range(2)]
    named = jnp.where(hits[0], 1.0, 0.0) + jnp.where(hits[1], 1.0, 0.0)
    above = lax.broadcasted_iota(jnp.int32, (rows, rows), 0)
    above = above > lax.broadcasted_iota(jnp.int32, (rows, rows), 1)
    ranks = jnp.dot(
        jnp.where(above, 1.0, 0.0).astype(jnp.bfloat16),
        named.astype(jnp.bfloat16),
        preferred_element_type=jnp.float32,
    )
    spots = ranks + (lane * cap).astype(jnp.float32)
    table = jnp.zeros((rows, 128), jnp.float32)
    for which in range(2):
        spot = jnp.sum(jnp.where(hits[which], spots, 0.0), axis=1, keepdims=True)
        table = jnp.where(lane == which, spot, table)
        table = jnp.where(lane == which + 2, weights[:, which : which + 1], table)
    table = jnp.concatenate([table, jnp.zeros((128 - rows, 128), jnp.float32)], axis=0)
    return table.T[0:8, :]


def head_units(heads_a, heads_b):
    half = heads_a // 2
    order = [("a", head) for head in range(half)]
    order += [("b", head) for head in range(heads_b)]
    return order + [("a", head) for head in range(half, heads_a)]


def chosen(me, units, for_a, for_b):
    value = for_b(units[0][1]) if units[0][0] == "b" else for_a(units[0][1])
    for at, (group, head) in enumerate(units):
        if at:
            value = jnp.where(me == at, for_a(head) if group == "a" else for_b(head), value)
    return value


def column(row):
    return jnp.broadcast_to(row, (8, row.shape[1])).T[:, 0:1]


def attend_block(chunk, block, queries, keys, values_t, heads, facts):
    pick, scale, mix, gain, valid, share = facts
    rows = queries.shape[1]
    key = lax.broadcasted_iota(jnp.int32, (chunk, 2 * chunk), 0)
    asks = lax.broadcasted_iota(jnp.int32, (chunk, 2 * chunk), 1)
    allowed = key <= jnp.where(asks >= chunk, asks - chunk, asks)
    for part in reversed(range(rows // chunk)):
        first = part * chunk
        before = block * rows + first
        length = before + chunk
        query = queries[block, first : first + chunk, :]
        picked = jnp.concatenate([query * pick[0], query * pick[1]], axis=0)
        scores = lax.dot_general(
            keys[0:length, :],
            picked,
            (((1,), (1,)), ((), ())),
            preferred_element_type=jnp.float32,
        )
        newest = jnp.where(allowed, scores[before:], NEG)
        if before:
            scores = jnp.concatenate([scores[:before], newest], axis=0)
        else:
            scores = newest
        top = jnp.max(scores, axis=0, keepdims=True)
        weights = jnp.exp2((scores - top) * scale)
        sums = jnp.sum(weights, axis=0, keepdims=True)
        found = jnp.dot(
            values_t[:, 0:length], weights.astype(jnp.bfloat16), preferred_element_type=jnp.float32
        )
        found = found / sums
        mixed = found[:, :chunk] - mix * found[:, chunk:]
        square = jnp.sum(mixed * mixed * valid, axis=0, keepdims=True) * share
        heads[block, :, first : first + chunk] = (
            mixed * lax.rsqrt(square + EPS) * gain * HEAD_SCALE
        ).astype(jnp.bfloat16)


def layer_kernel(
    places,
    chips,
    cap,
    units,
    qa_ref,
    ka_ref,
    va_ref,
    qb_ref,
    kb_ref,
    vb_ref,
    mix_a_ref,
    mix_b_ref,
    gain_a_ref,
    gain_b_ref,
    resid_ref,
    gain_ref,
    ids_ref,
    weights_ref,
    proj_a_hbm,
    proj_b_hbm,
    gate_hbm,
    up_hbm,
    down_hbm,
    out_ref,
    ready_q,
    ready_k,
    ready_v,
    ready_b,
    queries,
    keys,
    values_t,
    heads,
    joined,
    turned,
    proj,
    gate,
    up,
    down,
    term,
    table,
    mixed,
    normed,
    twin,
    chip_sum,
    sums,
    near,
    stage,
    piece,
    hidden,
    part,
    pair,
    finished,
    back,
    leave,
    last,
    ins,
    inr,
    outs,
    outr,
    ws,
    ms,
    mr,
    ts,
    tr,
    rs,
    rr,
    zs,
    zr,
    xs,
    xr,
    ps,
    pr,
    qs,
    qr,
    bs,
    br,
    ls,
    lr,
):
    place, turn = lax.axis_index("sp"), lax.axis_index("tp")
    chip, core = lax.div(turn, 2), lax.rem(turn, 2)
    other = 2 * chip + 1 - core
    rows, width = normed.shape
    slots = places * cap
    depth_a = proj_a_hbm.shape[0]
    pairs = (
        (proj_a_hbm, proj.at[0:depth_a]),
        (proj_b_hbm, proj.at[depth_a : proj.shape[0]]),
        (gate_hbm, gate),
        (up_hbm, up),
        (down_hbm, down),
    )
    loads = [pltpu.make_async_copy(src, dst, ws.at[at]) for at, (src, dst) in enumerate(pairs)]
    for load in loads:
        load.start()

    seq, wide = qa_ref.shape[0], qa_ref.shape[2]
    narrow = qb_ref.shape[1]
    for ref, kept in ((qa_ref, ready_q), (ka_ref, ready_k)):
        split = pltpu.einshape("abc->bac", ref[...])
        for head in range(split.shape[0]):
            kept[head] = split[head]
    split = pltpu.einshape("abc->bac", va_ref[...])
    for head in range(split.shape[0]):
        ready_v[head] = split[head].T
    for head in range(qb_ref.shape[0]):
        ready_b[head] = jnp.concatenate([qb_ref[head], kb_ref[head]], axis=0).T
    table[0] = route_table(ids_ref[...], weights_ref[...], cap)
    greet_routes(places, chips)

    spans, reach = [], {"a": 0, "b": depth_a}
    for group, head in units:
        tall = wide if group == "a" else narrow
        spans.append((reach[group] + head * tall, tall))

    def unit_parts(unit, sender):
        group, head = units[unit]
        first = sender * seq
        if not isinstance(sender, int):
            first = pl.multiple_of(first, seq)
        span = pl.ds(first, seq)
        if group == "a":
            return (
                (ready_q.at[head], queries.at[sender]),
                (ready_k.at[head], keys.at[span, :]),
                (ready_v.at[head], values_t.at[:, span]),
            )
        return (
            (ready_b.at[head], queries.at[sender]),
            (vb_ref.at[head], values_t.at[0:narrow, span]),
        )

    def in_copies(unit, sender, away):
        return [
            remote(src, dst, ins.at[away, at], inr.at[sender, at], sp=unit)
            for at, (src, dst) in enumerate(unit_parts(unit, sender))
        ]

    def out_copy(unit, block):
        start, tall = spans[unit]
        return remote(
            heads.at[block, 0:tall],
            joined.at[start : start + tall],
            outs.at[block],
            outr.at[unit],
            sp=block,
        )

    for away in reversed(range(1, places)):
        for unit in range(places):

            @pl.when(place == unit ^ away)
            def _():
                for copy in in_copies(unit, place, away):
                    copy.start()

    def swap_halves(sender):
        both = queries[sender].astype(jnp.float32)
        keys[sender * seq : (sender + 1) * seq, :] = pltpu.roll(both, narrow, 1).astype(
            jnp.bfloat16
        )

    for unit in range(places):

        @pl.when(place == unit)
        def _():
            packed = units[unit][0] == "b"
            for src, dst in unit_parts(unit, unit):
                dst[...] = src[...]
            if packed:
                values_t[narrow:wide, :] = jnp.zeros((wide - narrow, places * seq), jnp.bfloat16)
                swap_halves(unit)
            for away in reversed(range(1, places)):
                sender = unit ^ away
                for copy in in_copies(unit, sender, away):
                    copy.wait_recv()
                if packed:
                    swap_halves(sender)

    is_a = chosen(place, units, lambda head: 1, lambda head: 0) == 1
    lane = lax.broadcasted_iota(jnp.int32, (1, wide), 1)
    map_wide = jnp.where(is_a, wide // 2, narrow // 2)
    pick = []
    for which in range(2):
        inside = (lane >= which * map_wide) & (lane < (which + 1) * map_wide)
        pick.append(jnp.where(inside, 1.0, 0.0).astype(jnp.bfloat16))
    scale = jnp.where(
        is_a,
        math.log2(math.e) / math.sqrt(wide // 2),
        math.log2(math.e) / math.sqrt(narrow // 2),
    )
    share = jnp.where(is_a, 1.0 / wide, 1.0 / narrow)
    mix = chosen(place, units, lambda head: mix_a_ref[head], lambda head: mix_b_ref[head])
    padded = jnp.concatenate(
        [gain_b_ref[...], jnp.zeros((1, wide - narrow), jnp.float32)], axis=1
    )
    gain = column(jnp.where(is_a, gain_a_ref[...], padded))
    valid = column(jnp.where(lane < jnp.where(is_a, wide, narrow), 1.0, 0.0))
    facts = (pick, scale, mix, gain, valid, share)
    chunk = math.gcd(seq, 256)
    for block in reversed(range(places)):
        attend_block(chunk, block, queries, keys, values_t, heads, facts)
        for unit in range(places):

            @pl.when(place == unit)
            def _():
                if unit == block:
                    start, tall = spans[unit]
                    joined[start : start + tall, :] = heads[block, 0:tall, :]
                else:
                    out_copy(unit, block).start()

    others = list(range(1, chips))

    def peer(apart):
        return 2 * flipped(chip, apart) + core

    def table_copy(apart):
        return remote(
            table.at[0], table.at[apart], ms.at[apart], mr.at[apart], tp=peer(apart)
        )

    def twin_copy(apart):
        spot = term.at[apart, 1 - core]
        return remote(spot, twin.at[apart], ts.at[apart], tr.at[apart], tp=other)

    def sum_copy(apart):
        return remote(
            chip_sum.at[apart], sums.at[apart], rs.at[apart], rr.at[apart], tp=peer(apart)
        )

    def near_copy(apart):
        return remote(normed, near.at[apart], zs.at[apart], zr.at[apart], tp=peer(apart))

    def route_copy(apart, away):
        expert = flipped(place, away)
        return remote(
            stage.at[apart, expert],
            piece.at[apart, core, place],
            xs.at[apart, away],
            xr.at[apart, away],
            sp=expert,
        )

    def pair_copy(apart):
        spot = piece.at[apart, core]
        return remote(spot, spot, ps.at[apart], pr.at[apart], tp=other)

    def part_copy(apart):
        return remote(
            part.at[apart, 1 - core], pair.at[apart], qs.at[apart], qr.at[apart], tp=other
        )

    def back_copy(apart, away):
        home = flipped(place, away)
        return remote(
            finished.at[apart, home],
            back.at[apart, place],
            bs.at[apart, away],
            br.at[apart, away],
            sp=home,
        )

    def last_copy(apart):
        return remote(leave.at[apart], last.at[apart], ls.at[apart], lr.at[apart], tp=peer(apart))

    for apart in others:
        table_copy(apart).start()
    for unit in range(places):

        @pl.when(place != unit)
        def _():
            out_copy(unit, unit).wait_recv()

    for load in loads[:2]:
        load.wait()
    turned[...] = joined[...].T
    turns = list(reversed(others)) + [0]
    for apart in turns:
        first = pl.multiple_of(flipped(chip, apart) * (2 * rows), 2 * rows)
        given = turned[pl.ds(first, 2 * rows), :]
        summed = jnp.dot(given, proj[...], preferred_element_type=jnp.float32)
        term[apart] = summed.astype(jnp.bfloat16).reshape(2, rows, width)
        twin_copy(apart).start()
    total = resid_ref[...].astype(jnp.float32)
    for apart in turns:
        twin_copy(apart).wait_recv()
        both = term[apart, core].astype(jnp.float32) + twin[apart].astype(jnp.float32)
        if apart:
            chip_sum[apart] = both.astype(jnp.bfloat16)
            sum_copy(apart).start()
        else:
            total = total + both
    for apart in others:
        sum_copy(apart).wait_recv()
        total = total + sums[apart].astype(jnp.float32)
    mixed[...] = total
    normed[...] = rms_scaled(total, gain_ref[...]).astype(jnp.bfloat16)
    for apart in others:
        near_copy(apart).start()

    slot = lax.broadcasted_iota(jnp.int32, (rows, slots), 1).astype(jnp.float32)

    def columns(apart):
        full = jnp.concatenate([table[apart], jnp.zeros((120, 128), jnp.float32)], axis=0)
        return full.T[0:rows, :]

    def send_out(apart):
        if apart:
            table_copy(apart).wait_recv()
            near_copy(apart).wait_recv()
        held = near[apart] if apart else normed[...]
        known = columns(apart)
        spread = jnp.zeros((rows, slots), jnp.float32)
        for which in range(2):
            spread = spread + jnp.where(slot == known[:, which : which + 1], 1.0, 0.0)
        sent = lax.dot_general(
            spread.astype(jnp.bfloat16),
            held,
            (((0,), (0,)), ((), ())),
            preferred_element_type=jnp.float32,
        )
        stage[apart] = sent.astype(jnp.bfloat16).reshape(places, cap, width)
        for away in reversed(range(1, places)):
            route_copy(apart, away).start()
        piece[apart, core, place] = stage[apart, place]

    def run_expert(apart):
        for away in range(1, places):
            route_copy(apart, away).wait_recv()
        pair_copy(apart).start()
        if 0 < apart <= chips // 2:
            settle(apart - 1)
        pair_copy(apart).wait_recv()
        given = piece[apart].reshape(2 * slots, width)
        opened = jnp.dot(given, gate[...], preferred_element_type=jnp.float32)
        raised = jnp.dot(given, up[...], preferred_element_type=jnp.float32)
        hidden[...] = (jax.nn.silu(opened) * raised).astype(jnp.bfloat16)
        if apart + ahead < chips:
            send_out(apart + ahead)
        lowered = jnp.dot(hidden[...], down[...], preferred_element_type=jnp.float32)
        part[apart] = lowered.astype(jnp.bfloat16).reshape(2, slots, width)
        part_copy(apart).start()

    def settle(apart):
        part_copy(apart).wait_recv()
        both = part[apart, core].astype(jnp.float32) + pair[apart].astype(jnp.float32)
        finished[apart] = both.astype(jnp.bfloat16).reshape(places, cap, width)

    def send_back(apart):
        for away in reversed(range(1, places)):
            back_copy(apart, away).start()
        back[apart, place] = finished[apart, place]

    def gathered(apart):
        known = columns(apart)
        gather = jnp.zeros((rows, slots), jnp.float32)
        for which in range(2):
            own = known[:, which : which + 1]
            gather = gather + jnp.where(slot == own, known[:, which + 2 : which + 3], 0.0)
        high = gather.astype(jnp.bfloat16)
        low = (gather - high.astype(jnp.float32)).astype(jnp.bfloat16)
        for away in range(1, places):
            back_copy(apart, away).wait_recv()
        held = back[apart].reshape(slots, width)
        found = jnp.dot(high, held, preferred_element_type=jnp.float32)
        return found + jnp.dot(low, held, preferred_element_type=jnp.float32)

    ahead = min(3, chips)
    for apart in range(ahead):
        send_out(apart)
    for load in loads[2:]:
        load.wait()
    for apart in range(chips):
        run_expert(apart)
        if apart >= chips // 2:
            settle(apart)
            send_back(apart)
    nearer = list(range(1, chips // 2))
    for apart in nearer + [0]:
        send_back(apart)
    for apart in list(range(chips // 2, chips)) + nearer:
        leave[apart] = gathered(apart).astype(jnp.bfloat16)
        last_copy(apart).start()
    total = mixed[...] + gathered(0)
    for apart in others:
        last_copy(apart).wait_recv()
        total = total + last[apart].astype(jnp.float32)
    out_ref[...] = total.astype(jnp.bfloat16)
    for unit in range(places):

        @pl.when(place == unit)
        def _():
            for away in range(1, places):
                for copy in in_copies(unit ^ away, unit, away):
                    copy.wait_send()
                out_copy(unit, unit ^ away).wait_send()

    for apart in range(chips):
        twin_copy(apart).wait_send()
        pair_copy(apart).wait_send()
        part_copy(apart).wait_send()
        if apart:
            table_copy(apart).wait_send()
            sum_copy(apart).wait_send()
            near_copy(apart).wait_send()
            last_copy(apart).wait_send()
        for away in range(1, places):
            route_copy(apart, away).wait_send()
            back_copy(apart, away).wait_send()


def vmem(count):
    return [pl.BlockSpec(memory_space=pltpu.VMEM)] * count


def whole_layer(attention, resid, norm_gain, ids, weights, capacity, proj, experts):
    query_a, key_a, value_a, query_b, key_b, value_b, mix_a, mix_b, gain_a, gain_b = attention
    places, chips = lax.axis_size("sp"), lax.axis_size("tp") // 2
    rows, width = resid.shape
    seq, heads_a, wide = query_a.shape
    heads_b, narrow = query_b.shape[1:]
    deep = experts[0].shape[2]
    slots = places * capacity
    tall = proj[0].shape[0] + proj[1].shape[0]
    sems = pltpu.SemaphoreType.DMA
    units = head_units(heads_a, heads_b)

    def held(*shape):
        return pltpu.VMEM(shape, jnp.bfloat16)

    smem = [pl.BlockSpec(memory_space=pltpu.SMEM)] * 2
    return pl.pallas_call(
        functools.partial(layer_kernel, places, chips, capacity, units),
        out_shape=jax.ShapeDtypeStruct((rows, width), jnp.bfloat16),
        in_specs=vmem(6) + smem + vmem(6) + [pl.BlockSpec(memory_space=pl.ANY)] * 5,
        out_specs=vmem(1)[0],
        scratch_shapes=[
            held(heads_a, seq, wide),
            held(heads_a, seq, wide),
            held(heads_a, wide, seq),
            held(heads_b, seq, wide),
            held(places, seq, wide),
            held(places * seq, wide),
            held(wide, places * seq),
            held(places, wide, seq),
            held(tall, seq),
            held(seq, tall),
            held(tall, width),
            held(width, deep),
            held(width, deep),
            held(deep, width),
            held(chips, 2, rows, width),
            pltpu.VMEM((chips, 8, 128), jnp.float32),
            pltpu.VMEM((rows, width), jnp.float32),
            held(rows, width),
            held(chips, rows, width),
            held(chips, rows, width),
            held(chips, rows, width),
            held(chips, rows, width),
            held(chips, places, capacity, width),
            held(chips, 2, places, capacity, width),
            held(2 * slots, deep),
            held(chips, 2, slots, width),
            held(chips, slots, width),
            held(chips, places, capacity, width),
            held(chips, places, capacity, width),
            held(chips, rows, width),
            held(chips, rows, width),
            *[sems((places, 3))] * 2,
            *[sems((places,))] * 2,
            sems((5,)),
            *[sems((chips,))] * 8,
            *[sems((chips, places))] * 2,
            *[sems((chips,))] * 4,
            *[sems((chips, places))] * 2,
            *[sems((chips,))] * 2,
        ],
        compiler_params=pltpu.CompilerParams(
            collective_id=1, has_side_effects=True, vmem_limit_bytes=67043328
        ),
    )(
        query_a,
        key_a,
        value_a,
        *[jnp.transpose(value, (1, 2, 0)) for value in (query_b, key_b, value_b)],
        mix_a,
        mix_b,
        gain_a[None, :],
        gain_b[None, :],
        resid,
        norm_gain[None, :],
        ids.T,
        weights.T,
        *proj,
        *[expert[0] for expert in experts],
    )


def per_device(
    resid,
    query_a,
    key_a,
    value_a,
    query_b,
    key_b,
    value_b,
    mix_a,
    mix_b,
    head_gain_a,
    head_gain_b,
    proj_a,
    proj_b,
    norm_gain,
    route_ids,
    route_weights,
    expert_gate,
    expert_up,
    expert_down,
):
    sp_ways, tp_ways = lax.axis_size("sp"), lax.axis_size("tp")
    width = resid.shape[1]
    tok_rows = resid.shape[0]
    top_count = route_ids.shape[1]
    capacity = 3 * top_count * tok_rows // (2 * sp_ways)
    attention = (
        query_a,
        key_a,
        value_a,
        query_b,
        key_b,
        value_b,
        mix_a,
        mix_b,
        head_gain_a,
        head_gain_b,
    )
    wide, narrow = query_a.shape[2], query_b.shape[2]
    fits = query_a.shape[1] + query_b.shape[1] == sp_ways and wide == 128 == 2 * narrow
    fits = fits and wide == value_a.shape[2] and narrow == value_b.shape[2]
    paired = tp_ways % 2 == 0 and tp_ways & (tp_ways - 1) == 0 and sp_ways & (sp_ways - 1) == 0
    paired = paired and top_count == 2 and capacity % 16 == 0 and tok_rows <= 128
    if fits and paired:
        return whole_layer(
            attention,
            resid,
            norm_gain,
            route_ids,
            route_weights,
            capacity,
            (proj_a, proj_b),
            (expert_gate, expert_up, expert_down),
        )
    heads_out_a, heads_out_b = zigzag_heads(*attention)
    term = jnp.dot(heads_out_a, proj_a, preferred_element_type=jnp.float32)
    term = term + jnp.dot(heads_out_b, proj_b, preferred_element_type=jnp.float32)
    own_slots = slot_numbers(route_ids, sp_ways, capacity)
    mixed = resid.astype(jnp.float32) + lax.psum_scatter(
        lax.optimization_barrier(term.astype(jnp.bfloat16))
        .astype(jnp.float32)
        .astype(jnp.bfloat16),
        "tp",
        scatter_dimension=0,
        tiled=True,
    ).astype(jnp.float32)
    normed = rms_scaled(mixed, norm_gain).astype(jnp.bfloat16)
    lookup = jnp.arange(sp_ways * capacity, dtype=jnp.int32)[:, None]
    spread = jnp.zeros((sp_ways * capacity, tok_rows), jnp.float32)
    for which in range(top_count):
        spread = spread + (own_slots[:, which][None, :] == lookup).astype(jnp.float32)
    outgoing = jnp.dot(
        spread.astype(jnp.bfloat16), normed, preferred_element_type=jnp.float32
    ).astype(jnp.bfloat16)
    arrived = lax.all_to_all(
        outgoing.reshape(sp_ways, capacity, width), "sp", split_axis=0, concat_axis=0, tiled=True
    )
    piece = lax.all_gather(arrived.reshape(sp_ways * capacity, width), "tp", axis=0, tiled=True)
    gate = jnp.dot(piece, expert_gate[0], preferred_element_type=jnp.float32)
    upward = jnp.dot(piece, expert_up[0], preferred_element_type=jnp.float32)
    hidden = (jax.nn.silu(gate) * upward).astype(jnp.bfloat16)
    term = jnp.dot(hidden, expert_down[0], preferred_element_type=jnp.float32)
    summed = lax.psum_scatter(
        lax.optimization_barrier(term.astype(jnp.bfloat16))
        .astype(jnp.float32)
        .astype(jnp.bfloat16),
        "tp",
        scatter_dimension=0,
        tiled=True,
    )
    finished_rows = summed.reshape(sp_ways, capacity, width)
    back = lax.all_to_all(finished_rows, "sp", split_axis=0, concat_axis=0, tiled=True)
    picked = jnp.take(back.reshape(sp_ways * capacity, width), own_slots.reshape(-1), axis=0)
    picked = picked.reshape(tok_rows, top_count, width)
    output = mixed + jnp.sum(route_weights[:, :, None] * picked.astype(jnp.float32), axis=1)
    return output.astype(jnp.bfloat16)


def solution(mesh):
    placed = (
        P(("sp", "tp"), None),
        P("sp", "tp", None),
        P("sp", "tp", None),
        P("sp", "tp", None),
        P("sp", "tp", None),
        P("sp", "tp", None),
        P("sp", "tp", None),
        P("tp"),
        P("tp"),
        P(),
        P(),
        P("tp", None),
        P("tp", None),
        P(),
        P(("sp", "tp"), None),
        P(("sp", "tp"), None),
        P("sp", None, "tp"),
        P("sp", None, "tp"),
        P("sp", "tp", None),
    )
    return jax.shard_map(
        per_device, mesh=mesh, in_specs=placed, out_specs=P(("sp", "tp"), None), check_vma=False
    )
```

```python
import functools
import math

import jax
import jax.numpy as jnp
from jax import lax
from jax.experimental import pallas as pl
from jax.experimental.pallas import tpu as pltpu
from jax.sharding import PartitionSpec as P

EPS = 1e-06
NEG = -1e30
HEAD_SCALE = 1.0 - (0.8 - 0.6 * math.exp(-0.3))
KEY_STEP = 512


def partner(value, axis, apart):
    return lax.ppermute(value, axis, [(i, i ^ 1 << apart) for i in range(lax.axis_size(axis))])


def rms_scaled(values, gain):
    return values * lax.rsqrt(jnp.mean(values * values, axis=-1, keepdims=True) + EPS) * gain


def slot_numbers(route_rows, experts, capacity):
    count, top_count = route_rows.shape
    flat = route_rows.reshape(count * top_count)
    onehot = (flat[:, None] == jnp.arange(experts, dtype=jnp.int32)[None, :]).astype(jnp.int32)
    ranks = jnp.sum((jnp.cumsum(onehot, axis=0) - onehot) * onehot, axis=1)
    return (flat * capacity + ranks).reshape(count, top_count)


def empty_map(count, heads, width):
    return (
        jnp.zeros((count, heads, width), jnp.float32),
        jnp.full((heads, count), NEG, jnp.float32),
        jnp.zeros((heads, count), jnp.float32),
    )


def empty_group(query, value):
    return (
        empty_map(query.shape[0], query.shape[1], value.shape[2]),
        empty_map(query.shape[0], query.shape[1], value.shape[2]),
    )


def map_update(state, query, keys, values, allowed, scale):
    weighted, maximum, sums = state
    scores = jnp.einsum("qhd,khd->hqk", query, keys, preferred_element_type=jnp.float32) * scale
    scores = jnp.where(allowed[None], scores, NEG)
    fresh = jnp.maximum(maximum, jnp.max(scores, axis=2))
    weights = jnp.where(allowed[None], jnp.exp(scores - fresh[:, :, None]), 0.0)
    factor = jnp.exp(maximum - fresh)
    sums = sums * factor + jnp.sum(weights, axis=2)
    added = jnp.einsum(
        "hqk,khv->qhv", weights.astype(jnp.bfloat16), values, preferred_element_type=jnp.float32
    )
    weighted = weighted * jnp.transpose(factor)[:, :, None] + added
    return (weighted, fresh, sums)


def group_update(states, query, keys, values, allowed):
    width = query.shape[2] // 2
    scale = 1.0 / math.sqrt(width)
    return tuple(
        (
            map_update(
                states[which],
                query[:, :, which * width : (which + 1) * width],
                keys[:, :, which * width : (which + 1) * width],
                values,
                allowed,
                scale,
            )
            for which in range(2)
        )
    )


def set_update(carry, queries, pieces):
    rows_a, rows_b, query_pos = queries
    piece_key_a, piece_value_a, piece_key_b, piece_value_b = pieces
    length = piece_key_a.shape[0]
    step = math.gcd(length, KEY_STEP)
    latest = query_pos[-1]

    def inner(index, states):
        first = index * step

        def compute(current):
            keys_a = lax.dynamic_slice_in_dim(piece_key_a, first, step, 0)
            values_a = lax.dynamic_slice_in_dim(piece_value_a, first, step, 0)
            keys_b = lax.dynamic_slice_in_dim(piece_key_b, first, step, 0)
            values_b = lax.dynamic_slice_in_dim(piece_value_b, first, step, 0)
            key_pos = first + jnp.arange(step, dtype=jnp.int32)
            allowed = key_pos[None, :] <= query_pos[:, None]
            return (
                group_update(current[0], rows_a, keys_a, values_a, allowed),
                group_update(current[1], rows_b, keys_b, values_b, allowed),
            )

        return lax.cond(first <= latest, compute, lambda current: current, states)

    return lax.fori_loop(0, length // step, inner, carry)


def finish_group(states, mix, gain):
    outputs = [state[0] / jnp.transpose(state[2])[:, :, None] for state in states]
    mixed = outputs[0] - mix[None, :, None] * outputs[1]
    normed = rms_scaled(mixed, gain) * HEAD_SCALE
    return normed.astype(jnp.bfloat16).reshape(mixed.shape[0], -1)


def zigzag_heads(query_a, key_a, value_a, query_b, key_b, value_b, mix_a, mix_b, gain_a, gain_b):
    head_gain_a, head_gain_b = gain_a, gain_b
    seq_rows = query_a.shape[0]
    sp_ways = lax.axis_size("sp")
    place = lax.axis_index("sp")
    positions = place * seq_rows + jnp.arange(seq_rows, dtype=jnp.int32)
    levels = sp_ways.bit_length() - 1
    half = seq_rows // 2
    moved = jnp.concatenate(
        [query_a[half:].reshape(half, -1), query_b[half:].reshape(half, -1)], axis=1
    )
    for bit in range(levels):
        moved = partner(moved, "sp", bit)
    split_at = query_a.shape[1] * query_a.shape[2]
    far_a = moved[:, :split_at].reshape(half, query_a.shape[1], query_a.shape[2])
    far_b = moved[:, split_at:].reshape(half, query_b.shape[1], query_b.shape[2])
    far_pos = (sp_ways - 1 - place) * seq_rows + half + jnp.arange(half, dtype=jnp.int32)
    query_sets = ((query_a[:half], query_b[:half], positions[:half]), (far_a, far_b, far_pos))

    def fold_keys(carry, pieces):
        return tuple(
            (set_update(states, queries, pieces) for states, queries in zip(carry, query_sets))
        )

    initial = tuple(
        (
            (empty_group(queries[0], value_a), empty_group(queries[1], value_b))
            for queries in query_sets
        )
    )
    results = fold_keys(
        initial,
        (
            lax.all_gather(key_a, "sp", axis=0, tiled=True),
            lax.all_gather(value_a, "sp", axis=0, tiled=True),
            lax.all_gather(key_b, "sp", axis=0, tiled=True),
            lax.all_gather(value_b, "sp", axis=0, tiled=True),
        ),
    )
    finished = [
        (finish_group(states[0], mix_a, head_gain_a), finish_group(states[1], mix_b, head_gain_b))
        for states in results
    ]
    returned = jnp.concatenate([finished[1][0], finished[1][1]], axis=1)
    for bit in range(levels):
        returned = partner(returned, "sp", bit)
    width_a = finished[0][0].shape[1]
    heads_out_a = jnp.concatenate([finished[0][0], returned[:, :width_a]], axis=0)
    heads_out_b = jnp.concatenate([finished[0][1], returned[:, width_a:]], axis=0)
    return heads_out_a, heads_out_b


def remote(src, dst, send_sem, recv_sem, **where):
    return pltpu.make_async_remote_copy(
        src_ref=src,
        dst_ref=dst,
        send_sem=send_sem,
        recv_sem=recv_sem,
        device_id=where,
        device_id_type=pl.DeviceIdType.MESH,
    )


def greet_routes(places, chips):
    place, turn = lax.axis_index("sp"), lax.axis_index("tp")
    chip, core = lax.div(turn, 2), lax.rem(turn, 2)
    barrier = pltpu.get_barrier_semaphore()
    peers = [{"tp": 2 * chip + 1 - core}]
    peers += [{"tp": 2 * lax.rem(chip + apart, chips) + core} for apart in range(1, chips)]
    peers += [{"sp": lax.rem(place + apart, places)} for apart in range(1, places)]
    for peer in peers:
        pl.semaphore_signal(
            barrier, inc=1, device_id=peer, device_id_type=pl.DeviceIdType.MESH
        )
    return functools.partial(pl.semaphore_wait, barrier, len(peers))


def flipped(value, apart):
    bit = 1
    while bit <= apart:
        if apart & bit:
            value = value + bit - 2 * bit * lax.rem(lax.div(value, bit), 2)
        bit *= 2
    return value


def route_table(ids, weights, cap):
    rows = ids.shape[1]
    joined = [ids.astype(jnp.float32), weights, jnp.zeros((4, rows), jnp.float32)]
    full = jnp.concatenate(joined, axis=0)
    if rows < 128:
        full = jnp.concatenate([full, jnp.zeros((8, 128 - rows), jnp.float32)], axis=1)
    full = full.T[0:rows, :]
    ids, weights = full[:, 0:2].astype(jnp.int32), full[:, 2:4]
    lane = lax.broadcasted_iota(jnp.int32, (rows, 128), 1)
    hits = [ids[:, which : which + 1] == lane for which in range(2)]
    named = jnp.where(hits[0], 1.0, 0.0) + jnp.where(hits[1], 1.0, 0.0)
    above = lax.broadcasted_iota(jnp.int32, (rows, rows), 0)
    above = above > lax.broadcasted_iota(jnp.int32, (rows, rows), 1)
    ranks = jnp.dot(
        jnp.where(above, 1.0, 0.0).astype(jnp.bfloat16),
        named.astype(jnp.bfloat16),
        preferred_element_type=jnp.float32,
    )
    spots = ranks + (lane * cap).astype(jnp.float32)
    table = jnp.zeros((rows, 128), jnp.float32)
    for which in range(2):
        spot = jnp.sum(jnp.where(hits[which], spots, 0.0), axis=1, keepdims=True)
        table = jnp.where(lane == which, spot, table)
        table = jnp.where(lane == which + 2, weights[:, which : which + 1], table)
    table = jnp.concatenate([table, jnp.zeros((128 - rows, 128), jnp.float32)], axis=0)
    return table.T[0:8, :]


def head_units(heads_a, heads_b):
    half = heads_a // 2
    order = [("a", head) for head in range(half)]
    order += [("b", head) for head in range(heads_b)]
    return order + [("a", head) for head in range(half, heads_a)]


def chosen(me, units, for_a, for_b):
    value = for_b(units[0][1]) if units[0][0] == "b" else for_a(units[0][1])
    for at, (group, head) in enumerate(units):
        if at:
            value = jnp.where(me == at, for_a(head) if group == "a" else for_b(head), value)
    return value


def column(row):
    return jnp.broadcast_to(row, (8, row.shape[1])).T[:, 0:1]


def attend_block(chunk, block, queries, keys, values_t, heads, facts):
    pick, scale, mix, gain, valid, share = facts
    rows = queries.shape[1]
    key = lax.broadcasted_iota(jnp.int32, (chunk, 2 * chunk), 0)
    asks = lax.broadcasted_iota(jnp.int32, (chunk, 2 * chunk), 1)
    allowed = key <= jnp.where(asks >= chunk, asks - chunk, asks)
    for part in reversed(range(rows // chunk)):
        first = part * chunk
        before = block * rows + first
        length = before + chunk
        query = queries[block, first : first + chunk, :]
        picked = jnp.concatenate([query * pick[0], query * pick[1]], axis=0)
        scores = lax.dot_general(
            keys[0:length, :],
            picked,
            (((1,), (1,)), ((), ())),
            preferred_element_type=jnp.float32,
        )
        newest = jnp.where(allowed, scores[before:], NEG)
        if before:
            scores = jnp.concatenate([scores[:before], newest], axis=0)
        else:
            scores = newest
        top = jnp.max(scores, axis=0, keepdims=True)
        weights = jnp.exp2((scores - top) * scale)
        sums = jnp.sum(weights, axis=0, keepdims=True)
        found = jnp.dot(
            values_t[:, 0:length], weights.astype(jnp.bfloat16), preferred_element_type=jnp.float32
        )
        found = found / sums
        mixed = found[:, :chunk] - mix * found[:, chunk:]
        square = jnp.sum(mixed * mixed * valid, axis=0, keepdims=True) * share
        heads[block, :, first : first + chunk] = (
            mixed * lax.rsqrt(square + EPS) * gain * HEAD_SCALE
        ).astype(jnp.bfloat16)


def layer_kernel(
    places,
    chips,
    cap,
    units,
    qa_ref,
    ka_ref,
    va_ref,
    qb_ref,
    kb_ref,
    vb_ref,
    mix_a_ref,
    mix_b_ref,
    gain_a_ref,
    gain_b_ref,
    resid_ref,
    gain_ref,
    ids_ref,
    weights_ref,
    proj_a_hbm,
    proj_b_hbm,
    gate_hbm,
    up_hbm,
    down_hbm,
    out_ref,
    ready_q,
    ready_k,
    ready_v,
    ready_b,
    queries,
    keys,
    values_t,
    heads,
    joined,
    turned,
    proj,
    gate,
    up,
    down,
    term,
    table,
    mixed,
    normed,
    twin,
    chip_sum,
    sums,
    near,
    stage,
    piece,
    hidden,
    part,
    pair,
    finished,
    back,
    leave,
    last,
    ins,
    inr,
    outs,
    outr,
    ws,
    ms,
    mr,
    ts,
    tr,
    rs,
    rr,
    zs,
    zr,
    xs,
    xr,
    ps,
    pr,
    qs,
    qr,
    bs,
    br,
    ls,
    lr,
):
    place, turn = lax.axis_index("sp"), lax.axis_index("tp")
    chip, core = lax.div(turn, 2), lax.rem(turn, 2)
    other = 2 * chip + 1 - core
    rows, width = normed.shape
    slots = places * cap
    depth_a = proj_a_hbm.shape[0]
    pairs = (
        (proj_a_hbm, proj.at[0:depth_a]),
        (proj_b_hbm, proj.at[depth_a : proj.shape[0]]),
        (gate_hbm, gate),
        (up_hbm, up),
        (down_hbm, down),
    )
    loads = [pltpu.make_async_copy(src, dst, ws.at[at]) for at, (src, dst) in enumerate(pairs)]
    all_here = greet_routes(places, chips)
    for load in loads:
        load.start()

    seq, wide = qa_ref.shape[0], qa_ref.shape[2]
    narrow = qb_ref.shape[1]
    for ref, kept in ((qa_ref, ready_q), (ka_ref, ready_k)):
        split = pltpu.einshape("abc->bac", ref[...])
        for head in range(split.shape[0]):
            kept[head] = split[head]
    split = pltpu.einshape("abc->bac", va_ref[...])
    for head in range(split.shape[0]):
        ready_v[head] = split[head].T
    for head in range(qb_ref.shape[0]):
        ready_b[head] = jnp.concatenate([qb_ref[head], kb_ref[head]], axis=0).T
    table[0] = route_table(ids_ref[...], weights_ref[...], cap)
    all_here()

    spans, reach = [], {"a": 0, "b": depth_a}
    for group, head in units:
        tall = wide if group == "a" else narrow
        spans.append((reach[group] + head * tall, tall))

    def unit_parts(unit, sender):
        group, head = units[unit]
        first = sender * seq
        if not isinstance(sender, int):
            first = pl.multiple_of(first, seq)
        span = pl.ds(first, seq)
        if group == "a":
            return (
                (ready_q.at[head], queries.at[sender]),
                (ready_k.at[head], keys.at[span, :]),
                (ready_v.at[head], values_t.at[:, span]),
            )
        return (
            (ready_b.at[head], queries.at[sender]),
            (vb_ref.at[head], values_t.at[0:narrow, span]),
        )

    def in_copies(unit, sender, away):
        return [
            remote(src, dst, ins.at[away, at], inr.at[sender, at], sp=unit)
            for at, (src, dst) in enumerate(unit_parts(unit, sender))
        ]

    def out_copy(unit, block):
        start, tall = spans[unit]
        return remote(
            heads.at[block, 0:tall],
            joined.at[start : start + tall],
            outs.at[block],
            outr.at[unit],
            sp=block,
        )

    for away in reversed(range(1, places)):
        for unit in range(places):

            @pl.when(place == unit ^ away)
            def _():
                for copy in in_copies(unit, place, away):
                    copy.start()

    def swap_halves(sender):
        both = queries[sender].astype(jnp.float32)
        keys[sender * seq : (sender + 1) * seq, :] = pltpu.roll(both, narrow, 1).astype(
            jnp.bfloat16
        )

    for unit in range(places):

        @pl.when(place == unit)
        def _():
            packed = units[unit][0] == "b"
            for src, dst in unit_parts(unit, unit):
                dst[...] = src[...]
            if packed:
                values_t[narrow:wide, :] = jnp.zeros((wide - narrow, places * seq), jnp.bfloat16)
                swap_halves(unit)
            for away in reversed(range(1, places)):
                sender = unit ^ away
                for copy in in_copies(unit, sender, away):
                    copy.wait_recv()
                if packed:
                    swap_halves(sender)

    is_a = chosen(place, units, lambda head: 1, lambda head: 0) == 1
    lane = lax.broadcasted_iota(jnp.int32, (1, wide), 1)
    map_wide = jnp.where(is_a, wide // 2, narrow // 2)
    pick = []
    for which in range(2):
        inside = (lane >= which * map_wide) & (lane < (which + 1) * map_wide)
        pick.append(jnp.where(inside, 1.0, 0.0).astype(jnp.bfloat16))
    scale = jnp.where(
        is_a,
        math.log2(math.e) / math.sqrt(wide // 2),
        math.log2(math.e) / math.sqrt(narrow // 2),
    )
    share = jnp.where(is_a, 1.0 / wide, 1.0 / narrow)
    mix = chosen(place, units, lambda head: mix_a_ref[head], lambda head: mix_b_ref[head])
    padded = jnp.concatenate(
        [gain_b_ref[...], jnp.zeros((1, wide - narrow), jnp.float32)], axis=1
    )
    gain = column(jnp.where(is_a, gain_a_ref[...], padded))
    valid = column(jnp.where(lane < jnp.where(is_a, wide, narrow), 1.0, 0.0))
    facts = (pick, scale, mix, gain, valid, share)
    chunk = math.gcd(seq, 256)
    for block in reversed(range(places)):
        attend_block(chunk, block, queries, keys, values_t, heads, facts)
        for unit in range(places):

            @pl.when(place == unit)
            def _():
                if unit == block:
                    start, tall = spans[unit]
                    joined[start : start + tall, :] = heads[block, 0:tall, :]
                else:
                    out_copy(unit, block).start()

    others = list(range(1, chips))

    def peer(apart):
        return 2 * flipped(chip, apart) + core

    def table_copy(apart):
        return remote(
            table.at[0], table.at[apart], ms.at[apart], mr.at[apart], tp=peer(apart)
        )

    def twin_copy(apart):
        spot = term.at[apart, 1 - core]
        return remote(spot, twin.at[apart], ts.at[apart], tr.at[apart], tp=other)

    chunks = 2
    chunk_rows = rows // chunks

    def sum_copy(source, target, slot, to, lot):
        span = slice(lot * chunk_rows, (lot + 1) * chunk_rows)
        return remote(
            chip_sum.at[source, span],
            sums.at[target, span],
            rs.at[source, lot],
            rr.at[slot, lot],
            tp=peer(to),
        )

    def beside_copy(lot):
        return sum_copy(1, 1, 1, 1, lot)

    def relay_copy(apart, lot):
        return sum_copy(apart, apart ^ 1, apart ^ 1, 1, lot)

    def across_copy(apart, lot):
        return sum_copy(apart, 0, 0, apart, lot)

    def near_copy(apart):
        return remote(normed, near.at[apart], zs.at[apart], zr.at[apart], tp=peer(apart))

    def route_copy(apart, away):
        expert = flipped(place, away)
        return remote(
            stage.at[apart, expert],
            piece.at[apart, core, place],
            xs.at[apart, away],
            xr.at[apart, away],
            sp=expert,
        )

    def pair_copy(apart):
        spot = piece.at[apart, core]
        return remote(spot, spot, ps.at[apart], pr.at[apart], tp=other)

    def part_copy(apart):
        return remote(
            part.at[apart, 1 - core], pair.at[apart], qs.at[apart], qr.at[apart], tp=other
        )

    def back_copy(apart, away):
        home = flipped(place, away)
        return remote(
            finished.at[apart, home],
            back.at[apart, place],
            bs.at[apart, away],
            br.at[apart, away],
            sp=home,
        )

    def last_copy(apart):
        return remote(leave.at[apart], last.at[apart], ls.at[apart], lr.at[apart], tp=peer(apart))

    for apart in others:
        table_copy(apart).start()
    for unit in range(places):

        @pl.when(place != unit)
        def _():
            out_copy(unit, unit).wait_recv()

    for load in loads[:2]:
        load.wait()
    turned[...] = joined[...].T
    turns = list(reversed(others)) + [0]
    outer = (chip == 0) | (chip == chips - 1)
    for apart in turns:
        first = pl.multiple_of(flipped(chip, apart) * (2 * rows), 2 * rows)
        given = turned[pl.ds(first, 2 * rows), :]
        summed = jnp.dot(given, proj[...], preferred_element_type=jnp.float32)
        term[apart] = summed.astype(jnp.bfloat16).reshape(2, rows, width)
        twin_copy(apart).start()
    total = resid_ref[...].astype(jnp.float32)
    for apart in turns:
        twin_copy(apart).wait_recv()
        both = term[apart, core].astype(jnp.float32) + twin[apart].astype(jnp.float32)
        if apart:
            chip_sum[apart] = both.astype(jnp.bfloat16)
            for lot in range(chunks):
                if apart == 1:
                    beside_copy(lot).start()
                else:
                    pl.when(outer)(relay_copy(apart, lot).start)
        else:
            total = total + both

    @pl.when(jnp.logical_not(outer))
    def _():
        for apart in (2, 3):
            for lot in range(chunks):
                span = slice(lot * chunk_rows, (lot + 1) * chunk_rows)
                relay_copy(apart ^ 1, lot).wait_recv()
                both = chip_sum[apart, span, :].astype(jnp.float32)
                both = both + sums[apart, span, :].astype(jnp.float32)
                chip_sum[apart, span, :] = both.astype(jnp.bfloat16)
                across_copy(apart, lot).start()

    for lot in range(chunks):
        beside_copy(lot).wait_recv()
    total = total + sums[1].astype(jnp.float32)
    for lot in range(chunks):
        across_copy(2, lot).wait_recv()
    total = total + sums[0].astype(jnp.float32)
    mixed[...] = total
    normed[...] = rms_scaled(total, gain_ref[...]).astype(jnp.bfloat16)
    for apart in others:
        near_copy(apart).start()

    slot = lax.broadcasted_iota(jnp.int32, (rows, slots), 1).astype(jnp.float32)

    def columns(apart):
        full = jnp.concatenate([table[apart], jnp.zeros((120, 128), jnp.float32)], axis=0)
        return full.T[0:rows, :]

    def send_out(apart):
        if apart:
            table_copy(apart).wait_recv()
            near_copy(apart).wait_recv()
        held = near[apart] if apart else normed[...]
        known = columns(apart)
        spread = jnp.zeros((rows, slots), jnp.float32)
        for which in range(2):
            spread = spread + jnp.where(slot == known[:, which : which + 1], 1.0, 0.0)
        sent = lax.dot_general(
            spread.astype(jnp.bfloat16),
            held,
            (((0,), (0,)), ((), ())),
            preferred_element_type=jnp.float32,
        )
        stage[apart] = sent.astype(jnp.bfloat16).reshape(places, cap, width)
        for away in reversed(range(1, places)):
            route_copy(apart, away).start()
        piece[apart, core, place] = stage[apart, place]

    def run_expert(apart):
        for away in range(1, places):
            route_copy(apart, away).wait_recv()
        pair_copy(apart).start()
        if 0 < apart <= chips // 2:
            settle(apart - 1)
        pair_copy(apart).wait_recv()
        given = piece[apart].reshape(2 * slots, width)
        opened = jnp.dot(given, gate[...], preferred_element_type=jnp.float32)
        raised = jnp.dot(given, up[...], preferred_element_type=jnp.float32)
        hidden[...] = (jax.nn.silu(opened) * raised).astype(jnp.bfloat16)
        if apart + ahead < chips:
            send_out(apart + ahead)
        lowered = jnp.dot(hidden[...], down[...], preferred_element_type=jnp.float32)
        part[apart] = lowered.astype(jnp.bfloat16).reshape(2, slots, width)
        part_copy(apart).start()

    def settle(apart):
        part_copy(apart).wait_recv()
        both = part[apart, core].astype(jnp.float32) + pair[apart].astype(jnp.float32)
        finished[apart] = both.astype(jnp.bfloat16).reshape(places, cap, width)

    def send_back(apart):
        for away in reversed(range(1, places)):
            back_copy(apart, away).start()
        back[apart, place] = finished[apart, place]

    def gathered(apart):
        known = columns(apart)
        gather = jnp.zeros((rows, slots), jnp.float32)
        for which in range(2):
            own = known[:, which : which + 1]
            gather = gather + jnp.where(slot == own, known[:, which + 2 : which + 3], 0.0)
        high = gather.astype(jnp.bfloat16)
        low = (gather - high.astype(jnp.float32)).astype(jnp.bfloat16)
        for away in range(1, places):
            back_copy(apart, away).wait_recv()
        held = back[apart].reshape(slots, width)
        found = jnp.dot(high, held, preferred_element_type=jnp.float32)
        return found + jnp.dot(low, held, preferred_element_type=jnp.float32)

    ahead = min(3, chips)
    for apart in range(ahead):
        send_out(apart)
    for load in loads[2:]:
        load.wait()
    for apart in range(chips):
        run_expert(apart)
        if apart >= chips // 2:
            settle(apart)
            send_back(apart)
    nearer = list(range(1, chips // 2))
    for apart in nearer + [0]:
        send_back(apart)
    for apart in list(range(chips // 2, chips)) + nearer:
        leave[apart] = gathered(apart).astype(jnp.bfloat16)
        last_copy(apart).start()
    total = mixed[...] + gathered(0)
    for apart in others:
        last_copy(apart).wait_recv()
        total = total + last[apart].astype(jnp.float32)
    out_ref[...] = total.astype(jnp.bfloat16)
    for unit in range(places):

        @pl.when(place == unit)
        def _():
            for away in range(1, places):
                for copy in in_copies(unit ^ away, unit, away):
                    copy.wait_send()
                out_copy(unit, unit ^ away).wait_send()

    for apart in range(chips):
        twin_copy(apart).wait_send()
        pair_copy(apart).wait_send()
        part_copy(apart).wait_send()
        if apart:
            table_copy(apart).wait_send()
            for lot in range(chunks):
                across_copy(apart, lot).wait_send()
            near_copy(apart).wait_send()
            last_copy(apart).wait_send()
        for away in range(1, places):
            route_copy(apart, away).wait_send()
            back_copy(apart, away).wait_send()


def vmem(count):
    return [pl.BlockSpec(memory_space=pltpu.VMEM)] * count


def whole_layer(attention, resid, norm_gain, ids, weights, capacity, proj, experts):
    query_a, key_a, value_a, query_b, key_b, value_b, mix_a, mix_b, gain_a, gain_b = attention
    places, chips = lax.axis_size("sp"), lax.axis_size("tp") // 2
    rows, width = resid.shape
    seq, heads_a, wide = query_a.shape
    heads_b, narrow = query_b.shape[1:]
    deep = experts[0].shape[2]
    slots = places * capacity
    tall = proj[0].shape[0] + proj[1].shape[0]
    sems = pltpu.SemaphoreType.DMA
    units = head_units(heads_a, heads_b)

    def held(*shape):
        return pltpu.VMEM(shape, jnp.bfloat16)

    smem = [pl.BlockSpec(memory_space=pltpu.SMEM)] * 2
    return pl.pallas_call(
        functools.partial(layer_kernel, places, chips, capacity, units),
        out_shape=jax.ShapeDtypeStruct((rows, width), jnp.bfloat16),
        in_specs=vmem(6) + smem + vmem(6) + [pl.BlockSpec(memory_space=pl.ANY)] * 5,
        out_specs=vmem(1)[0],
        scratch_shapes=[
            held(heads_a, seq, wide),
            held(heads_a, seq, wide),
            held(heads_a, wide, seq),
            held(heads_b, seq, wide),
            held(places, seq, wide),
            held(places * seq, wide),
            held(wide, places * seq),
            held(places, wide, seq),
            held(tall, seq),
            held(seq, tall),
            held(tall, width),
            held(width, deep),
            held(width, deep),
            held(deep, width),
            held(chips, 2, rows, width),
            pltpu.VMEM((chips, 8, 128), jnp.float32),
            pltpu.VMEM((rows, width), jnp.float32),
            held(rows, width),
            held(chips, rows, width),
            held(chips, rows, width),
            held(chips, rows, width),
            held(chips, rows, width),
            held(chips, places, capacity, width),
            held(chips, 2, places, capacity, width),
            held(2 * slots, deep),
            held(chips, 2, slots, width),
            held(chips, slots, width),
            held(chips, places, capacity, width),
            held(chips, places, capacity, width),
            held(chips, rows, width),
            held(chips, rows, width),
            *[sems((places, 3))] * 2,
            *[sems((places,))] * 2,
            sems((5,)),
            *[sems((chips,))] * 4,
            *[sems((chips, 2))] * 2,
            *[sems((chips,))] * 2,
            *[sems((chips, places))] * 2,
            *[sems((chips,))] * 4,
            *[sems((chips, places))] * 2,
            *[sems((chips,))] * 2,
        ],
        compiler_params=pltpu.CompilerParams(
            collective_id=1, has_side_effects=True, vmem_limit_bytes=67043328
        ),
    )(
        query_a,
        key_a,
        value_a,
        *[jnp.transpose(value, (1, 2, 0)) for value in (query_b, key_b, value_b)],
        mix_a,
        mix_b,
        gain_a[None, :],
        gain_b[None, :],
        resid,
        norm_gain[None, :],
        ids.T,
        weights.T,
        *proj,
        *[expert[0] for expert in experts],
    )


def per_device(
    resid,
    query_a,
    key_a,
    value_a,
    query_b,
    key_b,
    value_b,
    mix_a,
    mix_b,
    head_gain_a,
    head_gain_b,
    proj_a,
    proj_b,
    norm_gain,
    route_ids,
    route_weights,
    expert_gate,
    expert_up,
    expert_down,
):
    sp_ways, tp_ways = lax.axis_size("sp"), lax.axis_size("tp")
    width = resid.shape[1]
    tok_rows = resid.shape[0]
    top_count = route_ids.shape[1]
    capacity = 3 * top_count * tok_rows // (2 * sp_ways)
    attention = (
        query_a,
        key_a,
        value_a,
        query_b,
        key_b,
        value_b,
        mix_a,
        mix_b,
        head_gain_a,
        head_gain_b,
    )
    wide, narrow = query_a.shape[2], query_b.shape[2]
    fits = query_a.shape[1] + query_b.shape[1] == sp_ways and wide == 128 == 2 * narrow
    fits = fits and wide == value_a.shape[2] and narrow == value_b.shape[2]
    paired = tp_ways % 2 == 0 and tp_ways & (tp_ways - 1) == 0 and sp_ways & (sp_ways - 1) == 0
    paired = paired and top_count == 2 and capacity % 16 == 0 and tok_rows <= 128
    if fits and paired and tp_ways == 8:
        return whole_layer(
            attention,
            resid,
            norm_gain,
            route_ids,
            route_weights,
            capacity,
            (proj_a, proj_b),
            (expert_gate, expert_up, expert_down),
        )
    heads_out_a, heads_out_b = zigzag_heads(*attention)
    term = jnp.dot(heads_out_a, proj_a, preferred_element_type=jnp.float32)
    term = term + jnp.dot(heads_out_b, proj_b, preferred_element_type=jnp.float32)
    own_slots = slot_numbers(route_ids, sp_ways, capacity)
    mixed = resid.astype(jnp.float32) + lax.psum_scatter(
        lax.optimization_barrier(term.astype(jnp.bfloat16))
        .astype(jnp.float32)
        .astype(jnp.bfloat16),
        "tp",
        scatter_dimension=0,
        tiled=True,
    ).astype(jnp.float32)
    normed = rms_scaled(mixed, norm_gain).astype(jnp.bfloat16)
    lookup = jnp.arange(sp_ways * capacity, dtype=jnp.int32)[:, None]
    spread = jnp.zeros((sp_ways * capacity, tok_rows), jnp.float32)
    for which in range(top_count):
        spread = spread + (own_slots[:, which][None, :] == lookup).astype(jnp.float32)
    outgoing = jnp.dot(
        spread.astype(jnp.bfloat16), normed, preferred_element_type=jnp.float32
    ).astype(jnp.bfloat16)
    arrived = lax.all_to_all(
        outgoing.reshape(sp_ways, capacity, width), "sp", split_axis=0, concat_axis=0, tiled=True
    )
    piece = lax.all_gather(arrived.reshape(sp_ways * capacity, width), "tp", axis=0, tiled=True)
    gate = jnp.dot(piece, expert_gate[0], preferred_element_type=jnp.float32)
    upward = jnp.dot(piece, expert_up[0], preferred_element_type=jnp.float32)
    hidden = (jax.nn.silu(gate) * upward).astype(jnp.bfloat16)
    term = jnp.dot(hidden, expert_down[0], preferred_element_type=jnp.float32)
    summed = lax.psum_scatter(
        lax.optimization_barrier(term.astype(jnp.bfloat16))
        .astype(jnp.float32)
        .astype(jnp.bfloat16),
        "tp",
        scatter_dimension=0,
        tiled=True,
    )
    finished_rows = summed.reshape(sp_ways, capacity, width)
    back = lax.all_to_all(finished_rows, "sp", split_axis=0, concat_axis=0, tiled=True)
    picked = jnp.take(back.reshape(sp_ways * capacity, width), own_slots.reshape(-1), axis=0)
    picked = picked.reshape(tok_rows, top_count, width)
    output = mixed + jnp.sum(route_weights[:, :, None] * picked.astype(jnp.float32), axis=1)
    return output.astype(jnp.bfloat16)


def solution(mesh):
    placed = (
        P(("sp", "tp"), None),
        P("sp", "tp", None),
        P("sp", "tp", None),
        P("sp", "tp", None),
        P("sp", "tp", None),
        P("sp", "tp", None),
        P("sp", "tp", None),
        P("tp"),
        P("tp"),
        P(),
        P(),
        P("tp", None),
        P("tp", None),
        P(),
        P(("sp", "tp"), None),
        P(("sp", "tp"), None),
        P("sp", None, "tp"),
        P("sp", None, "tp"),
        P("sp", "tp", None),
    )
    return jax.shard_map(
        per_device, mesh=mesh, in_specs=placed, out_specs=P(("sp", "tp"), None), check_vma=False
    )
```
